512 devices in a mesh: grp: 2 (over y), kv: 64 (over z, core), tp: 4 (over x).
Axes of the slice: x: 4, y: 2, z: 32, core: 2. Of those that a mesh axis runs over, the one named last changes fastest.
The devices are a block of a 4x8x32 slice.
Arguments:
- hidden_states: bfloat16 [128, 4096], P('grp', 'kv'), parts along dimension 0, may hold values from -6 to 6
- w_query: bfloat16 [4096, 2048], P('kv', 'tp'), may hold values from -0.09375 to 0.09375
- w_key: bfloat16 [4096, 2048], P('kv', 'tp'), may hold values from -0.09375 to 0.09375
- w_value: bfloat16 [4096, 2048], P('kv', 'tp'), may hold values from -0.09375 to 0.09375
- query_gain: float32 [64], replicated, may hold values from 1.2 to 1.8
- key_gain: float32 [64], replicated, may hold values from 1.2 to 1.8
- lambda_head: float32 [16], P('tp'), may hold values from 0.3 to 0.8
- head_gain: float32 [128], replicated, may hold values from 0.1 to 1.9
- w_output: bfloat16 [2048, 4096], P('tp', 'kv'), may hold values from -0.125 to 0.125
- cache_keys: bfloat16 [8, 16384, 16, 128], P('grp', 'kv', 'tp'), parts along dimension 0
- cache_values: bfloat16 [8, 16384, 16, 128], P('grp', 'kv', 'tp'), parts along dimension 0, may hold values from -6 to 6
- past_lengths: int32 [8], P('grp'), parts along dimension 0, may hold values from 8192 to 16352
- accepted: int32 [8], P('grp'), parts along dimension 0, may hold values from 1 to 8
- parents: int32 [8, 16], P('grp'), parts along dimension 0, may hold values from -1 to 14, as said below
Outputs:
- attended: bfloat16 [128, 4096], P(('grp', 'tp'), 'kv'), parts along dimension 0
- new_cache_keys: bfloat16 [8, 16384, 16, 128], P('grp', 'kv', 'tp'), parts along dimension 0
- new_cache_values: bfloat16 [8, 16384, 16, 128], P('grp', 'kv', 'tp'), parts along dimension 0
The draws below stay inside these ranges and needn't reach their ends.
There are 2 independent parts, one for each index of `grp`. The reference program is written for one: setup_inputs(seed, part) draws one part's arguments, and reference() takes and returns one part's arrays. A program takes and returns all parts, laid end to end along the dimension named above; an argument that names none is the same for every part. Nothing has to cross between parts.
Inputs may be any that keep to these rules, and one draw needn't show every extreme that they name: parents[s, 0] is -1 and parents[s, j] lies in 0 to j - 1 for j >= 1.
All inputs are finite; a program needn't handle non-finite values.
Results may differ from the reference program's by a relative error of at most 0.0095.
The reference program's roundings to bfloat16 on the way count: a program that leaves them out, or rounds other values in their place, can miss the bound.
Values may be sent and summed in bfloat16 or wider, within the bound.
No kernel may reach another device: no remote copies, remote signals or barrier semaphores. Data moves between devices by JAX's collectives and lax.ppermute only.
A program may use at most 64 MiB of HBM per device.

```python
import math
import jax
import jax.numpy as jnp
from jax import lax

D = 4096
HEADS = 16
HEAD_DIM = 64
VALUE_DIM = 128
PROP = 16
SEQS = 4
POS_DEV = 256
CACHE = 16384
TOKENS = 64
N_KV = 64
N_TP = 4


def draw_cache_keys(key, part):
    base = jax.random.normal(jax.random.fold_in(key, 11), (SEQS, CACHE, HEADS, 2 * HEAD_DIM), jnp.float32) * 1.4
    return base.astype(jnp.bfloat16)


def draw_parents(key, part):
    orders = jnp.arange(PROP, dtype=jnp.int32)
    picks = jax.random.randint(jax.random.fold_in(key, 21), (SEQS, PROP), 0, jnp.maximum(orders, 1)[None, :])
    return jnp.where(orders[None, :] == 0, -1, picks).astype(jnp.int32)


def with_ends(values, key, smallest, high):
    dims = values.shape
    place = [jax.random.randint(jax.random.fold_in(key, axis), (), 0, dims[axis]) for axis in range(len(dims))]
    values = values.at[tuple(place)].set(smallest)
    longest = dims.index(max(dims))
    place[longest] = (place[longest] + 1) % dims[longest]
    return values.at[tuple(place)].set(high)


def levels(stream_key, extent, cuts, least, top_value):
    gain = 1.0
    for axis_at, shards_of in cuts:
        draws = jax.random.uniform(jax.random.fold_in(jax.random.fold_in(stream_key, 6), axis_at), (shards_of,), jnp.float32, least / len(cuts), top_value / len(cuts))
        gain = gain * jnp.repeat(jnp.exp(draws), extent[axis_at] // shards_of).reshape((-1,) + (1,) * (len(extent) - 1 - axis_at))
    return gain


def gaussian(stream_key, dims, deviation, most, pieces=(), kind=jnp.bfloat16):
    loudness = levels(stream_key, dims, pieces, -0.22, 0.18) if pieces else 1.0
    result = jax.random.normal(stream_key, dims, jnp.float32) * deviation * loudness
    return jnp.minimum(jnp.maximum(result, -most), most).astype(kind)


def setup_inputs(seed: int = 0, part: int = 0) -> dict:
    streams_of = jax.random.split(jax.random.key(seed), 15)
    part_splits = jax.random.split(jax.random.fold_in(streams_of[14], part), 15)
    return {
        "hidden_states": gaussian(part_splits[0], (TOKENS, D), 1.0, 6.0, ((1, 64),)),
        "w_query": gaussian(streams_of[1], (D, HEADS * 2 * HEAD_DIM), D ** -0.5, 0.09375, ((0, 64), (1, 4))),
        "w_key": gaussian(streams_of[2], (D, HEADS * 2 * HEAD_DIM), D ** -0.5, 0.09375, ((0, 64), (1, 4))),
        "w_value": gaussian(streams_of[3], (D, HEADS * VALUE_DIM), D ** -0.5, 0.09375, ((0, 64), (1, 4))),
        "query_gain": jnp.clip(jnp.exp(jax.random.uniform(streams_of[4], (HEAD_DIM,), jnp.float32, math.log(1.2), math.log(1.8))), 1.2, 1.8),
        "key_gain": jnp.clip(jnp.exp(jax.random.uniform(streams_of[5], (HEAD_DIM,), jnp.float32, math.log(1.2), math.log(1.8))), 1.2, 1.8),
        "lambda_head": jnp.clip(0.3 + 0.5 * jax.random.uniform(streams_of[6], (HEADS,), jnp.float32) ** levels(streams_of[6], (HEADS,), ((0, 4),), -0.2, 0.2), 0.3, 0.8),
        "head_gain": jnp.clip(1.0 + 0.18 * jax.random.normal(streams_of[7], (VALUE_DIM,), jnp.float32), 0.1, 1.9),
        "w_output": gaussian(streams_of[8], (HEADS * VALUE_DIM, D), (HEADS * VALUE_DIM) ** -0.5, 0.125, ((0, 4), (1, 64))),
        "cache_keys": draw_cache_keys(jax.random.fold_in(jax.random.fold_in(streams_of[14], part), 71), part),
        "cache_values": gaussian(part_splits[10], (SEQS, CACHE, HEADS, VALUE_DIM), 1.0, 6.0, ((1, 64), (2, 4))),
        "past_lengths": with_ends(jax.random.randint(part_splits[11], (SEQS,), CACHE // 2, CACHE - 2 * PROP + 1), jax.random.fold_in(part_splits[11], 1), CACHE // 2, CACHE - 2 * PROP).astype(jnp.int32),
        "accepted": with_ends(jax.random.randint(part_splits[12], (SEQS,), 1, PROP // 2 + 1), jax.random.fold_in(part_splits[12], 1), 1, (PROP // 2 + 1) - 1).astype(jnp.int32),
        "parents": draw_parents(jax.random.fold_in(jax.random.fold_in(streams_of[14], part), 71), part),
    }


epsilon = 1e-06
floor_value = -1e+30

def group_norm(projected, gain_vector):
    shaped = projected.reshape(projected.shape[0], -1, gain_vector.shape[0])
    factor = lax.rsqrt(lax.optimization_barrier(jnp.mean(shaped * shaped, axis=-1, keepdims=True)) + epsilon)
    return (shaped * factor * gain_vector).reshape(projected.shape[0], -1)

def ancestry(parents):
    proposals = parents.shape[1]
    orders = jnp.arange(proposals, dtype=jnp.int32)
    reached = (parents[:, :, None] == orders[None, None, :]).astype(jnp.float32)
    reached = reached + (orders[:, None] == orders[None, :]).astype(jnp.float32)[None]
    for repeat in range((proposals - 1).bit_length()):
        reached = jnp.minimum(jnp.einsum('sjk,ski->sji', reached, reached, precision=lax.Precision.HIGHEST), 1.0)
    return reached

def reference(hidden_states, w_query, w_key, w_value, query_gain, key_gain, lambda_head, head_gain, w_output, cache_keys, cache_values, past_lengths, accepted, parents):
    query_terms = jnp.dot(hidden_states, w_query, preferred_element_type=jnp.float32)
    key_terms = jnp.dot(hidden_states, w_key, preferred_element_type=jnp.float32)
    value_terms = jnp.dot(hidden_states, w_value, preferred_element_type=jnp.float32)
    queries = group_norm(query_terms, query_gain).astype(jnp.bfloat16).reshape(SEQS, PROP, HEADS, 2, HEAD_DIM)
    keys_new = group_norm(key_terms, key_gain).astype(jnp.bfloat16).reshape(SEQS, PROP, HEADS, 2 * HEAD_DIM)
    values_new = value_terms.astype(jnp.bfloat16).reshape(SEQS, PROP, HEADS, VALUE_DIM)
    valid_len = past_lengths + accepted
    reached = ancestry(parents)
    score_scale = HEAD_DIM ** (-0.5)

    def one_sequence(inputs):
        query, key_rows, value_rows, cache_k, cache_v, length, reach_one = inputs
        blocks_k = cache_k.astype(jnp.float32).reshape(N_KV, POS_DEV, HEADS, 2, HEAD_DIM)
        blocks_v = cache_v.astype(jnp.float32).reshape(N_KV, POS_DEV, HEADS, VALUE_DIM)
        query_wide = query.astype(jnp.float32)
        scores = jnp.einsum('qhcd,bphcd->bqhcp', query_wide, blocks_k) * score_scale
        positions = jnp.arange(CACHE, dtype=jnp.int32).reshape(N_KV, 1, 1, 1, POS_DEV)
        visible = positions < length
        masked = jnp.where(visible, scores, floor_value)
        block_max = lax.optimization_barrier(jnp.max(masked, axis=-1))
        weights = jnp.where(visible, jnp.exp(masked - block_max[..., None]), 0.0)
        block_sum = lax.optimization_barrier(jnp.sum(weights, axis=-1))
        rounded = lax.optimization_barrier(weights.astype(jnp.bfloat16)).astype(jnp.float32)
        block_acc = jnp.einsum('bqhcp,bphv->bqhcv', rounded, blocks_v)
        tree_keys = key_rows.astype(jnp.float32).reshape(PROP, HEADS, 2, HEAD_DIM)
        tree_scores = jnp.einsum('qhcd,khcd->qhck', query_wide, tree_keys) * score_scale
        tree_visible = (reach_one > 0.5)[:, None, None, :]
        tree_masked = jnp.where(tree_visible, tree_scores, floor_value)
        tree_max = lax.optimization_barrier(jnp.max(tree_masked, axis=-1))
        tree_weights = jnp.where(tree_visible, jnp.exp(tree_masked - tree_max[..., None]), 0.0)
        tree_sum = lax.optimization_barrier(jnp.sum(tree_weights, axis=-1))
        tree_rounded = lax.optimization_barrier(tree_weights.astype(jnp.bfloat16)).astype(jnp.float32)
        tree_acc = jnp.einsum('qhck,khv->qhcv', tree_rounded, value_rows.astype(jnp.float32))
        highest = jnp.maximum(lax.optimization_barrier(jnp.max(block_max, axis=0)), tree_max)
        block_factor = jnp.exp(block_max - highest[None])
        tree_factor = jnp.exp(tree_max - highest)
        totals = lax.optimization_barrier(jnp.sum(block_sum * block_factor, axis=0)) + tree_sum * tree_factor
        combined = lax.optimization_barrier(jnp.sum(block_acc * block_factor[..., None], axis=0)) + tree_acc * tree_factor[..., None]
        first_map = combined[:, :, 0] / totals[:, :, 0:1]
        second_map = combined[:, :, 1] / totals[:, :, 1:2]
        mixture = first_map - lambda_head[None, :, None] * second_map
        factor = lax.rsqrt(lax.optimization_barrier(jnp.mean(mixture * mixture, axis=-1, keepdims=True)) + epsilon)
        return (mixture * factor * head_gain).astype(jnp.bfloat16).reshape(PROP, HEADS * VALUE_DIM)
    head_out = lax.map(one_sequence, (queries, keys_new, values_new, cache_keys, cache_values, valid_len, reached))
    head_out = head_out.reshape(SEQS * PROP, HEADS * VALUE_DIM)
    group_rows = HEADS * VALUE_DIM // N_TP
    grouped = head_out.astype(jnp.float32).reshape(SEQS * PROP, N_TP, group_rows)
    weights_out = w_output.astype(jnp.float32).reshape(N_TP, group_rows, D)
    partial_value = jnp.einsum('tgr,grd->gtd', grouped, weights_out)
    rounded_out = lax.optimization_barrier(partial_value.astype(jnp.bfloat16)).astype(jnp.float32)
    attended = lax.optimization_barrier(jnp.sum(rounded_out, axis=0)).astype(jnp.bfloat16)

    def write_one(cache_rows, new_rows, first_row):
        zero_index = jnp.zeros((), jnp.int32)
        return lax.dynamic_update_slice(cache_rows, new_rows, (first_row.astype(jnp.int32), zero_index, zero_index))
    new_cache_keys = jax.vmap(write_one)(cache_keys, keys_new, valid_len)
    new_cache_values = jax.vmap(write_one)(cache_values, values_new, valid_len)
    return (attended, new_cache_keys, new_cache_values)
```

```python
import functools
import math

import jax
import jax.numpy as jnp
from jax import lax
from jax.experimental import pallas as pl
from jax.experimental.pallas import tpu as pltpu
from jax.sharding import Mesh
from jax.sharding import PartitionSpec as P

epsilon = 1e-06
floor_value = -1e30
f32 = jnp.float32
bf16 = jnp.bfloat16
interpreted = False
near_chips = 4
near_cores = 2
far, chip, core, tp = "far", "chip", "core", "tp"
near = (chip, core)
near_terms = 2
far_terms = 2

vmem = pl.BlockSpec(memory_space=pltpu.VMEM)
smem = pl.BlockSpec(memory_space=pltpu.SMEM)
anywhere = pl.BlockSpec(memory_space=pl.ANY)


def iota(shape, dim):
    return lax.broadcasted_iota(jnp.int32, shape, dim)


def call(body, out_shape, in_specs, out_specs=vmem, flops=1000000, room=4, **rest):
    return pl.pallas_call(
        body,
        out_shape=out_shape,
        in_specs=in_specs,
        out_specs=out_specs,
        interpret=interpreted,
        compiler_params=pltpu.CompilerParams(vmem_limit_bytes=room << 20),
        cost_estimate=pl.CostEstimate(flops=flops, bytes_accessed=1000000, transcendentals=0),
        **rest,
    )


def terms_of(x, count):
    terms = []
    for _ in range(count):
        terms.append(x.astype(bf16))
        x = x - terms[-1].astype(f32)
    return terms


def parts_of(x):
    high = x.astype(bf16).astype(f32)
    middle = (x - high).astype(bf16).astype(f32)
    return high, middle, x - high - middle


def project(hidden_ref, query_ref, key_ref, value_ref, out_ref):
    hidden = hidden_ref[...]
    width = query_ref.shape[1]
    at = 0
    for ref, count in ((query_ref, near_terms), (key_ref, 1), (value_ref, 1)):
        sums = jnp.dot(hidden, ref[...], preferred_element_type=f32)
        for term in terms_of(sums, count):
            out_ref[:, at : at + width] = term
            at += width


def arrived_sum(arrived_ref, width, terms):
    total = arrived_ref[0].astype(f32)
    for k in range(1, arrived_ref.shape[0]):
        total = total + arrived_ref[k].astype(f32)
    query = total[:, :width]
    for k in range(1, terms):
        query = query + total[:, k * width : (k + 1) * width]
    return query, total[:, terms * width :]


def sum_near(arrived_ref, out_ref, *, width):
    query, rest = arrived_sum(arrived_ref, width, near_terms)
    terms = terms_of(query, far_terms)
    for k in range(out_ref.shape[0]):
        for i, term in enumerate(terms):
            out_ref[k, :, i * width : (i + 1) * width] = term
        row = [rest[k : k + 1, 128 * i : 128 * (i + 1)] for i in range(8)]
        out_ref[k, :, far_terms * width :] = jnp.concatenate(row, axis=0).astype(bf16)


def normed(x, gain, lane, half):
    squares = x * x
    first = jnp.sum(jnp.where(lane < half, squares, 0.0), axis=-1, keepdims=True)
    second = jnp.sum(jnp.where(lane < half, 0.0, squares), axis=-1, keepdims=True)
    mean = jnp.where(lane < half, first, second) / half
    return x * lax.rsqrt(mean + epsilon) * gain


def finish_rows(arrived_ref, query_gain_ref, key_gain_ref, query_ref, row_ref):
    width = query_ref.shape[2]
    total, row = arrived_sum(arrived_ref, width, far_terms)
    lane = iota((8, 128), 1)
    for i in range(width // 128):
        at = slice(128 * i, 128 * (i + 1))
        part = normed(total[:, at], query_gain_ref[...], lane, 64).astype(bf16)
        for k in range(query_ref.shape[0]):
            query_ref[k, :, at] = part
    row = jnp.where(iota((8, 128), 0) < 4, normed(row, key_gain_ref[...], lane, 64), row)
    row_ref[...] = row.astype(bf16)


def attend(
    place_ref,
    past_ref,
    accepted_ref,
    parents_ref,
    lambda_ref,
    query_ref,
    row_ref,
    keys_ref,
    values_ref,
    out_ref,
    keys_out_ref,
    values_out_ref,
    sems,
):
    keys_copy = pltpu.make_async_copy(keys_ref, keys_out_ref, sems.at[0])
    values_copy = pltpu.make_async_copy(values_ref, values_out_ref, sems.at[1])
    keys_copy.start()
    values_copy.start()
    own, offset = place_ref[0], place_ref[1]
    seqs, proposals = parents_ref.shape
    own_seq, own_order = own // proposals, lax.rem(own, proposals)
    below = jnp.int32(0)
    for j in range(proposals):
        parent = parents_ref[own_seq, j]
        above = jnp.where(parent >= 0, (below >> jnp.maximum(parent, 0)) & 1, 0)
        below = below | (jnp.where(own_order == j, 1, above) << j)
    rows, columns = 128, keys_ref.shape[1]
    row = iota((rows, 128), 0)
    lane = iota((rows, 128), 1)
    row_head, row_comp = row & 3, (row >> 3) & 1
    row_order = 2 * (row >> 4) + ((row >> 2) & 1)
    spread = (iota((rows, proposals), 1) == row_order[:, :proposals]).astype(bf16)
    head_at = [row_head == h for h in range(4)]
    comp_at = (lane >= 64) == (row_comp == 1)
    line = iota((rows, columns), 0)
    column = iota((rows, columns), 1)
    same_head = (column & 3) == (line & 3)
    position = offset + (column >> 2)
    under = ((below >> row_order[:, :1]) & 1) == 1
    scale = jnp.ones((rows, 1), f32)
    for h in range(4):
        mine = (row_head[:, :1] == h) & (row_comp[:, :1] == 1)
        scale = jnp.where(mine, lambda_ref[h], scale)
    new_row = row_ref[...].astype(f32)
    new_key = jnp.concatenate([new_row[:4]] * (rows // 4), axis=0)
    new_value = jnp.concatenate([new_row[4:]] * (rows // 4), axis=0)
    for s in range(seqs):
        wide = jnp.dot(
            spread, query_ref[s * proposals : (s + 1) * proposals, :], preferred_element_type=f32
        )
        query = jnp.zeros((rows, 128), f32)
        for h in range(4):
            query = jnp.where(head_at[h], wide[:, 128 * h : 128 * (h + 1)], query)
        query = jnp.where(comp_at, query, 0.0)
        scores = lax.dot_general(
            query.astype(bf16),
            keys_ref[s],
            (((1,), (1,)), ((), ())),
            preferred_element_type=f32,
        )
        visible = same_head & (position < past_ref[s] + accepted_ref[s])
        masked = jnp.where(visible, scores * 0.125, floor_value)
        tree_score = jnp.sum(query * new_key, axis=-1, keepdims=True) * 0.125
        tree_visible = under & (own_seq == s)
        tree_masked = jnp.where(tree_visible, tree_score, floor_value)
        top = jnp.maximum(jnp.max(masked, axis=-1, keepdims=True), tree_masked)
        weights = jnp.where(visible, jnp.exp(masked - top), 0.0)
        tree_weight = jnp.where(tree_visible, jnp.exp(tree_masked - top), 0.0)
        total = jnp.sum(weights, axis=-1, keepdims=True) + tree_weight
        acc = jnp.dot(weights.astype(bf16), values_ref[s], preferred_element_type=f32)
        acc = (acc + tree_weight.astype(bf16).astype(f32) * new_value) * scale
        acc = acc.astype(bf16)
        stats = jnp.zeros((rows, 128), f32)
        for k, part in enumerate((*parts_of(top), *parts_of(total))):
            stats = jnp.where(lane == k, part, stats)
        stats = jnp.transpose(stats)[:8].astype(bf16)
        for r in range(out_ref.shape[0]):
            out_ref[r, s, :16, :] = acc[16 * r : 16 * (r + 1)]
            out_ref[r, s, 16:, :] = stats
    keys_copy.wait()
    values_copy.wait()


def stat_rows(stats):
    return stats[0:1] + stats[1:2] + stats[2:3], stats[3:4] + stats[4:5] + stats[5:6]


def combine_near(place_ref, arrived_ref, row_ref, out_ref, factor_ref):
    me = place_ref[2]
    sources, groups = arrived_ref.shape[:2]
    tiles, factors = [], []
    lane = iota((8, 128), 1)
    packed = jnp.zeros((8, 128), f32)
    for g in range(groups):
        tops, sums = zip(*[stat_rows(arrived_ref[r, g, 16:, :].astype(f32)) for r in range(sources)])
        top = functools.reduce(jnp.maximum, tops)
        scales = [jnp.exp(t - top) for t in tops]
        total = sum(s * f for s, f in zip(sums, scales))
        factors.extend(scales)
        zero = jnp.zeros((1, 128), f32)
        stats = jnp.concatenate([*parts_of(top), *parts_of(total), zero, zero], axis=0)
        moved = pltpu.roll(stats, lax.rem(128 + 16 * g - 16 * me, 128), 1)
        packed = jnp.where((lane >> 4) == g, moved, packed)
    count = sources * groups
    wide = jnp.concatenate(factors + [jnp.zeros((128 - count, 128), f32)], axis=0)
    factor_ref[...] = jnp.transpose(wide)
    mine = factor_ref[pl.ds(pl.multiple_of(16 * me, 16), 16), :]
    for g in range(groups):
        acc = jnp.zeros((16, 128), f32)
        for r in range(sources):
            at = g * sources + r
            acc = acc + arrived_ref[r, g, :16, :].astype(f32) * mine[:, at : at + 1]
        tiles.append(acc.astype(bf16))
    for k in range(out_ref.shape[0]):
        for g in range(groups):
            out_ref[k, 16 * g : 16 * (g + 1), :] = tiles[g]
        out_ref[k, 64:72, :] = packed.astype(bf16)
        out_ref[k, 72:80, :] = row_ref[...]


def combine_far(arrived_ref, gain_ref, out_ref):
    sources = arrived_ref.shape[0]
    tops, sums = zip(*[stat_rows(arrived_ref[q, 64:72, :].astype(f32)) for q in range(sources)])
    top = functools.reduce(jnp.maximum, tops)
    scales = [jnp.exp(t - top) for t in tops]
    total = sum(s * f for s, f in zip(sums, scales))
    wide = jnp.concatenate(scales + [total, jnp.zeros((127 - sources, 128), f32)], axis=0)
    columns = jnp.transpose(wide)[:64]
    acc = jnp.zeros((64, 128), f32)
    for q in range(sources):
        acc = acc + arrived_ref[q, :64, :].astype(f32) * columns[:, q : q + 1]
    acc = acc / columns[:, sources : sources + 1]
    heads = []
    for g in range(4):
        mixture = acc[16 * g : 16 * g + 8] - acc[16 * g + 8 : 16 * g + 16]
        mean = jnp.mean(mixture * mixture, axis=-1, keepdims=True)
        heads.append((mixture * lax.rsqrt(mean + epsilon) * gain_ref[...]).astype(bf16))
    for k in range(out_ref.shape[0]):
        for g in range(4):
            out_ref[k, 8 * g : 8 * (g + 1), :] = heads[g]
        for q in range(sources):
            out_ref[k, 32 + 8 * q : 40 + 8 * q, :] = arrived_ref[q, 72:80, :]


def finish(
    place_ref,
    past_ref,
    accepted_ref,
    arrived_ref,
    weight_ref,
    keys_ref,
    values_ref,
    out_ref,
    keys_out_ref,
    values_out_ref,
    key_rows,
    value_rows,
    sem,
):
    del keys_ref, values_ref
    sources = arrived_ref.shape[0]
    heads = jnp.concatenate([arrived_ref[r, :32, :] for r in range(sources)], axis=0)
    count = heads.shape[0]
    to = iota((count, count), 0)
    source = ((to >> 1) & 7) * 32 + (to >> 6) * 8 + (to & 1) * 4 + ((to >> 4) & 3)
    order = (iota((count, count), 1) == source).astype(bf16)
    heads = jnp.dot(order, heads, preferred_element_type=f32).astype(bf16)
    total = jnp.zeros(out_ref.shape, f32)
    for g in range(4):
        left = jnp.concatenate(
            [heads[64 * g + 16 * h : 64 * g + 16 * (h + 1)] for h in range(4)], axis=1
        )
        group = lax.dot_general(
            left, weight_ref[g], (((1,), (1,)), ((), ())), preferred_element_type=f32
        )
        total = total + group.astype(bf16).astype(f32)
    out_ref[...] = total.astype(bf16)
    offset = place_ref[1]
    seqs, positions_dev = keys_out_ref.shape[:2]
    proposals = key_rows.shape[0]
    for s in range(seqs):
        first = past_ref[s] + accepted_ref[s] - offset

        @pl.when((first > -proposals) & (first < positions_dev))
        def _():
            for j in range(proposals):
                r, q = divmod(s * proposals + j, sources)
                key_rows[j] = arrived_ref[r, 32 + 8 * q : 36 + 8 * q, :]
                value_rows[j] = arrived_ref[r, 36 + 8 * q : 40 + 8 * q, :]
            for j in range(proposals):

                @pl.when((first + j >= 0) & (first + j < positions_dev))
                def _():
                    at = jnp.clip(first + j, 0, positions_dev - 1)
                    copies = [
                        pltpu.make_async_copy(rows.at[j], whole.at[s, at], sem.at[k])
                        for k, (rows, whole) in enumerate(
                            ((key_rows, keys_out_ref), (value_rows, values_out_ref))
                        )
                    ]
                    for c in copies:
                        c.start()
                    for c in copies:
                        c.wait()


def on_device(
    hidden_states,
    w_query,
    w_key,
    w_value,
    query_gain,
    key_gain,
    lambda_head,
    head_gain,
    w_output,
    cache_keys,
    cache_values,
    past_lengths,
    accepted,
    parents,
):
    shape = jax.ShapeDtypeStruct
    seqs, proposals = parents.shape
    tokens = hidden_states.shape[0]
    width = w_query.shape[1]
    positions_dev, heads = cache_keys.shape[1:3]
    nears, fars, tps = (math.prod(lax.axis_size(a) for a in axes) for axes in (near, (far,), (tp,)))
    chunk = tokens // nears
    near_index, far_index = lax.axis_index(near), lax.axis_index(far)
    shard = far_index * nears + near_index
    place = jnp.stack([near_index * chunk + far_index, shard * positions_dev, near_index])
    place = place.astype(jnp.int32)
    two_query = jnp.concatenate([query_gain, query_gain])[None]
    two_key = jnp.concatenate([key_gain, key_gain])[None]

    terms = call(project, shape((tokens, (near_terms + 2) * width), bf16), [vmem] * 4)(
        hidden_states, w_query, w_key, w_value
    )
    terms = lax.all_to_all(
        terms.reshape(nears, chunk, -1), near, 0, 0, tiled=True
    )
    shared = call(
        functools.partial(sum_near, width=width),
        shape((fars, chunk, far_terms * width + 128), bf16),
        [vmem],
    )(terms)
    shared = lax.all_to_all(shared, far, 0, 0, tiled=True)
    query, row = call(
        finish_rows,
        (shape((nears, chunk, width), bf16), shape((8, 128), bf16)),
        [vmem] * 3,
        (vmem, vmem),
    )(shared, two_query, two_key)
    query = lax.all_to_all(query, near, 0, 0, tiled=True).reshape(tokens, width)
    flat = (seqs, positions_dev * heads, 128)
    part, keys_copy, values_copy = call(
        attend,
        (
            shape((nears, tps, 24, 128), bf16),
            shape(flat, bf16),
            shape(flat, bf16),
        ),
        [smem] * 5 + [vmem] * 4,
        (vmem, anywhere, anywhere),
        scratch_shapes=[pltpu.SemaphoreType.DMA((2,))],
        flops=10000000,
        room=16,
    )(
        place,
        past_lengths,
        accepted,
        parents,
        lambda_head,
        query,
        row,
        cache_keys.reshape(flat),
        cache_values.reshape(flat),
    )
    part = lax.all_to_all(
        part.reshape(nears * tps, 24, 128), (*near, tp), 0, 0, tiled=True
    )
    part = call(
        combine_near,
        shape((fars, 80, 128), bf16),
        [smem, vmem, vmem],
        scratch_shapes=[pltpu.VMEM((128, 128), f32)],
    )(place, part.reshape(nears, tps, 24, 128), row)
    part = lax.all_to_all(part, far, 0, 0, tiled=True)
    mixed = call(combine_far, shape((nears, 96, 128), bf16), [vmem] * 2)(part, head_gain[None])
    mixed = lax.all_to_all(mixed, near, 0, 0, tiled=True)
    weight = jnp.broadcast_to(w_output.T[None], (tps, *w_output.T.shape))
    weight = lax.all_to_all(weight, tp, 0, 0, tiled=True)
    whole = cache_keys.shape
    return call(
        finish,
        (
            shape((proposals, w_output.shape[1]), bf16),
            shape(whole, bf16),
            shape(whole, bf16),
        ),
        [smem] * 3 + [vmem] * 2 + [anywhere] * 2,
        (vmem, anywhere, anywhere),
        scratch_shapes=[
            pltpu.VMEM((proposals, heads, 128), bf16),
            pltpu.VMEM((proposals, heads, 128), bf16),
            pltpu.SemaphoreType.DMA((2,)),
        ],
        input_output_aliases={5: 1, 6: 2},
    )(
        place,
        past_lengths,
        accepted,
        mixed,
        weight,
        keys_copy.reshape(whole),
        values_copy.reshape(whole),
    )


def solution(mesh):
    groups, shards, tps = (mesh.shape[a] for a in ("grp", "kv", "tp"))
    split = (groups, shards // (near_chips * near_cores), near_chips, near_cores, tps)
    finer = Mesh(mesh.devices.reshape(split), ("grp", far, chip, core, tp))
    kv = (far, chip, core)
    cache = P("grp", kv, tp, None)
    placed = (
        P("grp", kv),
        P(kv, tp),
        P(kv, tp),
        P(kv, tp),
        P(),
        P(),
        P(tp),
        P(),
        P(tp, kv),
        cache,
        cache,
        P("grp"),
        P("grp"),
        P("grp", None),
    )
    return jax.shard_map(
        on_device,
        mesh=finer,
        in_specs=placed,
        out_specs=(P(("grp", tp), kv), cache, cache),
        check_vma=False,
    )
```

```python
import functools
import math

import jax
import jax.numpy as jnp
from jax import lax
from jax.experimental import pallas as pl
from jax.experimental.pallas import tpu as pltpu
from jax.sharding import Mesh
from jax.sharding import PartitionSpec as P


epsilon = 1e-06
floor_value = -1e30
f32 = jnp.float32
bf16 = jnp.bfloat16
interpreted = False
near_chips = 4
near_cores = 2
far, chip, core, tp = "far", "chip", "core", "tp"
near = (chip, core)
near_terms = 2
far_terms = 2
rows = 128

vmem = pl.BlockSpec(memory_space=pltpu.VMEM)
smem = pl.BlockSpec(memory_space=pltpu.SMEM)
hbm = pl.BlockSpec(memory_space=pltpu.HBM)


def near_place():
    return lax.axis_index(chip) * lax.axis_size(core) + lax.axis_index(core)


def iota(shape, dim):
    return lax.broadcasted_iota(jnp.int32, shape, dim)


def call(body, out_shape, in_specs, out_specs=vmem, flops=1000000, room=4, **rest):
    return pl.pallas_call(
        body,
        out_shape=out_shape,
        in_specs=in_specs,
        out_specs=out_specs,
        interpret=interpreted,
        compiler_params=pltpu.CompilerParams(vmem_limit_bytes=room << 20),
        cost_estimate=pl.CostEstimate(flops=flops, bytes_accessed=1000000, transcendentals=0),
        **rest,
    )


def terms_of(x, count):
    terms = []
    for _ in range(count):
        terms.append(x.astype(bf16))
        x = x - terms[-1].astype(f32)
    return terms


def parts_of(x):
    high = x.astype(bf16).astype(f32)
    middle = (x - high).astype(bf16).astype(f32)
    return high, middle, x - high - middle


def project(hidden_ref, query_ref, key_ref, value_ref, out_ref, hidden, weights, sems):
    width = query_ref.shape[1]
    copies = [pltpu.make_async_copy(hidden_ref, hidden, sems.at[3])]
    for k, ref in enumerate((query_ref, key_ref, value_ref)):
        copies.append(pltpu.make_async_copy(ref, weights.at[k], sems.at[k]))
    for c in copies:
        c.start()
    at = 0
    copies[0].wait()
    for k, count in enumerate((near_terms, 1, 1)):
        copies[k + 1].wait()
        sums = jnp.dot(hidden[...], weights[k], preferred_element_type=f32)
        for term in terms_of(sums, count):
            out_ref[:, at : at + width] = term
            at += width


def arrived_sum(arrived_ref, width, terms):
    total = arrived_ref[0].astype(f32)
    for k in range(1, arrived_ref.shape[0]):
        total = total + arrived_ref[k].astype(f32)
    query = total[:, :width]
    for k in range(1, terms):
        query = query + total[:, k * width : (k + 1) * width]
    return query, total[:, terms * width :]


def sum_near(arrived_ref, out_ref, *, width):
    query, rest = arrived_sum(arrived_ref, width, near_terms)
    terms = terms_of(query, far_terms)
    for k in range(out_ref.shape[0]):
        for i, term in enumerate(terms):
            out_ref[k, :, i * width : (i + 1) * width] = term
        row = [rest[k : k + 1, 128 * i : 128 * (i + 1)] for i in range(8)]
        out_ref[k, :, far_terms * width :] = jnp.concatenate(row, axis=0).astype(bf16)


def normed(x, gain, lane, half):
    squares = x * x
    first = jnp.sum(jnp.where(lane < half, squares, 0.0), axis=-1, keepdims=True)
    second = jnp.sum(jnp.where(lane < half, 0.0, squares), axis=-1, keepdims=True)
    mean = jnp.where(lane < half, first, second) / half
    return x * lax.rsqrt(mean + epsilon) * gain


def finish_rows(arrived_ref, query_gain_ref, key_gain_ref, query_ref, row_ref):
    width = query_ref.shape[2]
    total, row = arrived_sum(arrived_ref, width, far_terms)
    lane = iota((8, 128), 1)
    query_gain = jnp.concatenate([query_gain_ref[...]] * 2, axis=1)
    key_gain = jnp.concatenate([key_gain_ref[...]] * 2, axis=1)
    for i in range(width // 128):
        at = slice(128 * i, 128 * (i + 1))
        part = normed(total[:, at], query_gain, lane, 64).astype(bf16)
        for k in range(query_ref.shape[0]):
            query_ref[k, :, at] = part
    row = jnp.where(iota((8, 128), 0) < 4, normed(row, key_gain, lane, 64), row)
    row_ref[...] = row.astype(bf16)


def stage(
    past_ref,
    accepted_ref,
    parents_ref,
    lambda_ref,
    keys_ref,
    values_ref,
    keys_vmem_ref,
    values_vmem_ref,
    keys_out_ref,
    values_out_ref,
    limit_ref,
    under_ref,
    scale_ref,
    sems,
):
    taken = [
        pltpu.make_async_copy(keys_ref, keys_vmem_ref, sems.at[0]),
        pltpu.make_async_copy(values_ref, values_vmem_ref, sems.at[1]),
    ]
    put = [
        pltpu.make_async_copy(keys_vmem_ref, keys_out_ref, sems.at[2]),
        pltpu.make_async_copy(values_vmem_ref, values_out_ref, sems.at[3]),
    ]
    for c in taken:
        c.start()
    seqs, proposals = parents_ref.shape
    nears = lax.axis_size(near)
    far_index = lax.axis_index(far)
    own = near_place() * (seqs * proposals // nears) + far_index
    offset = (far_index * nears + near_place()) * (keys_ref.shape[1] // 4)
    own_seq, own_order = own // proposals, lax.rem(own, proposals)
    below = jnp.int32(0)
    for j in range(proposals):
        parent = parents_ref[own_seq, j]
        above = jnp.where(parent >= 0, (below >> jnp.maximum(parent, 0)) & 1, 0)
        below = below | (jnp.where(own_order == j, 1, above) << j)
    row = iota((rows, 128), 0)
    under = (below >> (2 * (row >> 4) + ((row >> 2) & 1))) & 1
    limit = jnp.zeros((8, 128), jnp.int32)
    for s in range(seqs):
        limit = jnp.where(iota((8, 128), 0) == s, past_ref[s] + accepted_ref[s] - offset, limit)
        under_ref[s] = jnp.where(own_seq == s, under, 0).astype(f32)
    limit_ref[...] = limit
    scale = jnp.ones((rows, 128), f32)
    for h in range(4):
        scale = jnp.where(((row & 3) == h) & (((row >> 3) & 1) == 1), lambda_ref[h], scale)
    scale_ref[...] = scale
    for c, d in zip(taken, put):
        c.wait()
        d.start()
    for d in put:
        d.wait()


def attend(
    limit_ref,
    under_ref,
    scale_ref,
    query_ref,
    row_ref,
    keys_ref,
    values_ref,
    out_ref,
):
    seqs, columns = keys_ref.shape[:2]
    proposals = query_ref.shape[0] // seqs
    row = iota((rows, 128), 0)
    lane = iota((rows, 128), 1)
    row_head, row_comp = row & 3, (row >> 3) & 1
    row_order = 2 * (row >> 4) + ((row >> 2) & 1)
    spread = (iota((rows, proposals), 1) == row_order[:, :proposals]).astype(bf16)
    head_at = [row_head == h for h in range(4)]
    comp_at = (lane >= 64) == (row_comp == 1)
    column = iota((rows, columns), 1)
    same_head = (column & 3) == (iota((rows, columns), 0) & 3)
    position = jnp.where(same_head, column >> 2, columns)
    scale = scale_ref[...]
    new_row = row_ref[...].astype(f32)
    new_key = jnp.concatenate([new_row[:4]] * (rows // 4), axis=0)
    new_value = jnp.concatenate([new_row[4:]] * (rows // 4), axis=0)
    for s in range(seqs):
        wide = jnp.dot(
            spread, query_ref[s * proposals : (s + 1) * proposals, :], preferred_element_type=f32
        )
        query = jnp.zeros((rows, 128), f32)
        for h in range(4):
            query = jnp.where(head_at[h], wide[:, 128 * h : 128 * (h + 1)], query)
        query = jnp.where(comp_at, query, 0.0)
        scores = lax.dot_general(
            query.astype(bf16),
            keys_ref[s],
            (((1,), (1,)), ((), ())),
            preferred_element_type=f32,
        )
        visible = position < jnp.minimum(limit_ref[s : s + 1, :1], columns)
        masked = jnp.where(visible, scores * 0.125, floor_value)
        tree_score = jnp.sum(query * new_key, axis=-1, keepdims=True) * 0.125
        tree_visible = under_ref[s, :, :1] > 0.5
        tree_masked = jnp.where(tree_visible, tree_score, floor_value)
        top = jnp.maximum(jnp.max(masked, axis=-1, keepdims=True), tree_masked)
        weights = jnp.where(visible, jnp.exp(masked - top), 0.0)
        tree_weight = jnp.where(tree_visible, jnp.exp(tree_masked - top), 0.0)
        total = jnp.sum(weights, axis=-1, keepdims=True) + tree_weight
        acc = jnp.dot(weights.astype(bf16), values_ref[s], preferred_element_type=f32)
        acc = (acc + tree_weight.astype(bf16).astype(f32) * new_value) * scale
        acc = acc.astype(bf16)
        stats = jnp.zeros((rows, 128), f32)
        for k, part in enumerate((*parts_of(top), *parts_of(total))):
            stats = jnp.where(lane == k, part, stats)
        stats = jnp.transpose(stats)[:8].astype(bf16)
        for r in range(out_ref.shape[0]):
            out_ref[r, s, :16, :] = acc[16 * r : 16 * (r + 1)]
            out_ref[r, s, 16:, :] = stats


def stat_rows(stats):
    return stats[0:1] + stats[1:2] + stats[2:3], stats[3:4] + stats[4:5] + stats[5:6]


def combine_near(arrived_ref, row_ref, out_ref, factor_ref):
    me = near_place()
    sources, groups = arrived_ref.shape[:2]
    tiles, factors = [], []
    lane = iota((8, 128), 1)
    packed = jnp.zeros((8, 128), f32)
    for g in range(groups):
        tops, sums = zip(*[stat_rows(arrived_ref[r, g, 16:, :].astype(f32)) for r in range(sources)])
        top = functools.reduce(jnp.maximum, tops)
        scales = [jnp.exp(t - top) for t in tops]
        total = sum(s * f for s, f in zip(sums, scales))
        factors.extend(scales)
        zero = jnp.zeros((1, 128), f32)
        stats = jnp.concatenate([*parts_of(top), *parts_of(total), zero, zero], axis=0)
        moved = pltpu.roll(stats, lax.rem(128 + 16 * g - 16 * me, 128), 1)
        packed = jnp.where((lane >> 4) == g, moved, packed)
    count = sources * groups
    wide = jnp.concatenate(factors + [jnp.zeros((128 - count, 128), f32)], axis=0)
    factor_ref[...] = jnp.transpose(wide)
    mine = factor_ref[pl.ds(pl.multiple_of(16 * me, 16), 16), :]
    for g in range(groups):
        acc = jnp.zeros((16, 128), f32)
        for r in range(sources):
            at = g * sources + r
            acc = acc + arrived_ref[r, g, :16, :].astype(f32) * mine[:, at : at + 1]
        tiles.append(acc.astype(bf16))
    for k in range(out_ref.shape[0]):
        for g in range(groups):
            out_ref[k, 16 * g : 16 * (g + 1), :] = tiles[g]
        out_ref[k, 64:72, :] = packed.astype(bf16)
        out_ref[k, 72:80, :] = row_ref[...]


def combine_far(arrived_ref, gain_ref, out_ref):
    sources = arrived_ref.shape[0]
    tops, sums = zip(*[stat_rows(arrived_ref[q, 64:72, :].astype(f32)) for q in range(sources)])
    top = functools.reduce(jnp.maximum, tops)
    scales = [jnp.exp(t - top) for t in tops]
    total = sum(s * f for s, f in zip(sums, scales))
    wide = jnp.concatenate(scales + [total, jnp.zeros((127 - sources, 128), f32)], axis=0)
    columns = jnp.transpose(wide)[:64]
    acc = jnp.zeros((64, 128), f32)
    for q in range(sources):
        acc = acc + arrived_ref[q, :64, :].astype(f32) * columns[:, q : q + 1]
    acc = acc / columns[:, sources : sources + 1]
    heads = []
    for g in range(4):
        mixture = acc[16 * g : 16 * g + 8] - acc[16 * g + 8 : 16 * g + 16]
        mean = jnp.mean(mixture * mixture, axis=-1, keepdims=True)
        heads.append((mixture * lax.rsqrt(mean + epsilon) * gain_ref[...]).astype(bf16))
    for k in range(out_ref.shape[0]):
        for g in range(4):
            out_ref[k, 8 * g : 8 * (g + 1), :] = heads[g]
        for q in range(sources):
            out_ref[k, 32 + 8 * q : 40 + 8 * q, :] = arrived_ref[q, 72:80, :]


def finish(
    past_ref,
    accepted_ref,
    arrived_ref,
    own_ref,
    first_ref,
    second_ref,
    third_ref,
    keys_ref,
    values_ref,
    out_ref,
    keys_out_ref,
    values_out_ref,
    heads_ref,
    key_rows,
    value_rows,
    lengths,
    sem,
):
    known = [
        pltpu.make_async_copy(past_ref, lengths.at[0], sem.at[0]),
        pltpu.make_async_copy(accepted_ref, lengths.at[1], sem.at[1]),
    ]
    for c in known:
        c.start()
    del keys_ref, values_ref
    sources = arrived_ref.shape[0]
    heads = jnp.concatenate([arrived_ref[r, :32, :] for r in range(sources)], axis=0)
    count = heads.shape[0]
    to = iota((count, count), 0)
    source = ((to >> 1) & 7) * 32 + (to >> 6) * 8 + (to & 1) * 4 + ((to >> 4) & 3)
    order = (iota((count, count), 1) == source).astype(bf16)
    heads_ref[...] = jnp.dot(order, heads, preferred_element_type=f32)
    total = jnp.zeros(out_ref.shape, f32)
    for k, weight_ref in enumerate((own_ref, first_ref, second_ref, third_ref)):
        g = lax.rem(lax.axis_index(tp) + 4 - k, 4)
        mine = heads_ref[pl.ds(pl.multiple_of(64 * g, 64), 64), :].astype(bf16)
        left = jnp.concatenate([mine[16 * h : 16 * (h + 1)] for h in range(4)], axis=1)
        group = lax.dot_general(
            left, weight_ref[...], (((1,), (1,)), ((), ())), preferred_element_type=f32
        )
        total = total + group.astype(bf16).astype(f32)
    out_ref[...] = total.astype(bf16)
    for c in known:
        c.wait()
    seqs, positions_dev = keys_out_ref.shape[:2]
    offset = (lax.axis_index(far) * lax.axis_size(near) + near_place()) * positions_dev
    proposals = key_rows.shape[0]
    for s in range(seqs):
        first = lengths[0, s] + lengths[1, s] - offset

        @pl.when((first > -proposals) & (first < positions_dev))
        def _():
            for j in range(proposals):
                r, q = divmod(s * proposals + j, sources)
                key_rows[j] = arrived_ref[r, 32 + 8 * q : 36 + 8 * q, :]
                value_rows[j] = arrived_ref[r, 36 + 8 * q : 40 + 8 * q, :]
            for j in range(proposals):

                @pl.when((first + j >= 0) & (first + j < positions_dev))
                def _():
                    at = jnp.clip(first + j, 0, positions_dev - 1)
                    writes = [
                        pltpu.make_async_copy(rows.at[j], whole.at[s, at], sem.at[k])
                        for k, (rows, whole) in enumerate(
                            ((key_rows, keys_out_ref), (value_rows, values_out_ref))
                        )
                    ]
                    for c in writes:
                        c.start()
                    for c in writes:
                        c.wait()


def on_device(
    hidden_states,
    w_query,
    w_key,
    w_value,
    query_gain,
    key_gain,
    lambda_head,
    head_gain,
    w_output,
    cache_keys,
    cache_values,
    past_lengths,
    accepted,
    parents,
):
    shape = jax.ShapeDtypeStruct
    seqs, proposals = parents.shape
    tokens = hidden_states.shape[0]
    width = w_query.shape[1]
    positions_dev, heads = cache_keys.shape[1:3]
    nears, fars, tps = (math.prod(lax.axis_size(a) for a in axes) for axes in (near, (far,), (tp,)))
    chunk = tokens // nears
    terms = call(
        project,
        shape((tokens, (near_terms + 2) * width), bf16),
        [hbm] * 4,
        scratch_shapes=[
            pltpu.VMEM(hidden_states.shape, bf16),
            pltpu.VMEM((3, *w_query.shape), bf16),
            pltpu.SemaphoreType.DMA((4,)),
        ],
    )(hidden_states, w_query, w_key, w_value)
    terms = lax.all_to_all(
        terms.reshape(nears, chunk, -1), near, 0, 0, tiled=True
    )
    shared = call(
        functools.partial(sum_near, width=width),
        shape((fars, chunk, far_terms * width + 128), bf16),
        [vmem],
    )(terms)
    shared = lax.all_to_all(shared, far, 0, 0, tiled=True)
    query, row = call(
        finish_rows,
        (shape((nears, chunk, width), bf16), shape((8, 128), bf16)),
        [vmem] * 3,
        (vmem, vmem),
    )(shared, query_gain[None], key_gain[None])
    query = lax.all_to_all(query, near, 0, 0, tiled=True).reshape(tokens, width)
    flat = (seqs, positions_dev * heads, 128)
    keys, values, keys_copy, values_copy, limit, under, scale = call(
        stage,
        (
            *[shape(flat, bf16)] * 4,
            shape((8, 128), jnp.int32),
            shape((seqs, rows, 128), f32),
            shape((rows, 128), f32),
        ),
        [smem] * 4 + [hbm] * 2,
        (vmem, vmem, hbm, hbm, vmem, vmem, vmem),
        scratch_shapes=[pltpu.SemaphoreType.DMA((4,))],
    )(
        past_lengths,
        accepted,
        parents,
        lambda_head,
        cache_keys.reshape(flat),
        cache_values.reshape(flat),
    )
    part = call(
        attend, shape((nears, tps, 24, 128), bf16), [vmem] * 7, flops=10000000, room=16
    )(limit, under, scale, query, row, keys, values)
    part = lax.all_to_all(
        part.reshape(nears * tps, 24, 128), (*near, tp), 0, 0, tiled=True
    )
    part = call(
        combine_near,
        shape((fars, 80, 128), bf16),
        [vmem, vmem],
        scratch_shapes=[pltpu.VMEM((128, 128), f32)],
    )(part.reshape(nears, tps, 24, 128), row)
    part = lax.all_to_all(part, far, 0, 0, tiled=True)
    mixed = call(combine_far, shape((nears, 96, 128), bf16), [vmem] * 2)(part, head_gain[None])
    mixed = lax.all_to_all(mixed, near, 0, 0, tiled=True)
    own = w_output.T
    weights = [own]
    for k in range(1, tps):
        ring = [(i, (i + k) % tps) for i in range(tps)]
        weights.append(lax.ppermute(own, tp, ring))
    whole = cache_keys.shape
    return call(
        finish,
        (
            shape((proposals, w_output.shape[1]), bf16),
            shape(whole, bf16),
            shape(whole, bf16),
        ),
        [hbm] * 2 + [vmem] * 5 + [hbm] * 2,
        (vmem, hbm, hbm),
        scratch_shapes=[
            pltpu.VMEM((256, 128), f32),
            pltpu.VMEM((proposals, heads, 128), bf16),
            pltpu.VMEM((proposals, heads, 128), bf16),
            pltpu.SMEM((2, seqs), jnp.int32),
            pltpu.SemaphoreType.DMA((2,)),
        ],
        input_output_aliases={7: 1, 8: 2},
    )(past_lengths, accepted, mixed, *weights, keys_copy.reshape(whole), values_copy.reshape(whole))


def solution(mesh):
    groups, shards, tps = (mesh.shape[a] for a in ("grp", "kv", "tp"))
    split = (groups, shards // (near_chips * near_cores), near_chips, near_cores, tps)
    finer = Mesh(mesh.devices.reshape(split), ("grp", far, chip, core, tp))
    kv = (far, chip, core)
    cache = P("grp", kv, tp, None)
    placed = (
        P("grp", kv),
        P(kv, tp),
        P(kv, tp),
        P(kv, tp),
        P(),
        P(),
        P(tp),
        P(),
        P(tp, kv),
        cache,
        cache,
        P("grp"),
        P("grp"),
        P("grp", None),
    )
    return jax.shard_map(
        on_device,
        mesh=finer,
        in_specs=placed,
        out_specs=(P(("grp", tp), kv), cache, cache),
        check_vma=False,
    )
```

```python
import functools
import math

import jax
import jax.numpy as jnp
from jax import lax
from jax.experimental import pallas as pl
from jax.experimental.pallas import tpu as pltpu
from jax.sharding import Mesh
from jax.sharding import PartitionSpec as P


epsilon = 1e-06
floor_value = -1e30
f32 = jnp.float32
bf16 = jnp.bfloat16
interpreted = False
near_chips = 4
near_cores = 2
far, chip, core, tp = "far", "chip", "core", "tp"
near = (chip, core)
near_terms = 2
far_terms = 2
rows = 128

vmem = pl.BlockSpec(memory_space=pltpu.VMEM)
smem = pl.BlockSpec(memory_space=pltpu.SMEM)
hbm = pl.BlockSpec(memory_space=pltpu.HBM)


def near_place():
    return lax.axis_index(chip) * lax.axis_size(core) + lax.axis_index(core)


def iota(shape, dim):
    return lax.broadcasted_iota(jnp.int32, shape, dim)


def call(body, out_shape, in_specs, out_specs=vmem, flops=1000000, room=4, **rest):
    return pl.pallas_call(
        body,
        out_shape=out_shape,
        in_specs=in_specs,
        out_specs=out_specs,
        interpret=interpreted,
        compiler_params=pltpu.CompilerParams(vmem_limit_bytes=int(room * 1024) << 10),
        cost_estimate=pl.CostEstimate(flops=flops, bytes_accessed=1000000, transcendentals=0),
        **rest,
    )


def terms_of(x, count):
    terms = []
    for _ in range(count):
        terms.append(x.astype(bf16))
        x = x - terms[-1].astype(f32)
    return terms


def parts_of(x):
    high = x.astype(bf16).astype(f32)
    middle = (x - high).astype(bf16).astype(f32)
    return high, middle, x - high - middle


def project(hidden_ref, query_ref, key_ref, value_ref, out_ref, hidden, weights, sems):
    width = query_ref.shape[1]
    copies = [pltpu.make_async_copy(hidden_ref, hidden, sems.at[3])]
    for k, ref in enumerate((query_ref, key_ref, value_ref)):
        copies.append(pltpu.make_async_copy(ref, weights.at[k], sems.at[k]))
    for c in copies:
        c.start()
    at = 0
    copies[0].wait()
    for k, count in enumerate((near_terms, 1, 1)):
        copies[k + 1].wait()
        sums = jnp.dot(hidden[...], weights[k], preferred_element_type=f32)
        for term in terms_of(sums, count):
            out_ref[:, at : at + width] = term
            at += width


def arrived_sum(arrived_ref, width, terms):
    total = arrived_ref[0].astype(f32)
    for k in range(1, arrived_ref.shape[0]):
        total = total + arrived_ref[k].astype(f32)
    query = total[:, :width]
    for k in range(1, terms):
        query = query + total[:, k * width : (k + 1) * width]
    return query, total[:, terms * width :]


def sum_near(arrived_ref, out_ref, *, width):
    query, rest = arrived_sum(arrived_ref, width, near_terms)
    terms = terms_of(query, far_terms)
    for k in range(out_ref.shape[0]):
        for i, term in enumerate(terms):
            out_ref[k, :, i * width : (i + 1) * width] = term
        row = [rest[k : k + 1, 128 * i : 128 * (i + 1)] for i in range(8)]
        out_ref[k, :, far_terms * width :] = jnp.concatenate(row, axis=0).astype(bf16)


def normed(x, gain, lane, half):
    squares = x * x
    first = jnp.sum(jnp.where(lane < half, squares, 0.0), axis=-1, keepdims=True)
    second = jnp.sum(jnp.where(lane < half, 0.0, squares), axis=-1, keepdims=True)
    mean = jnp.where(lane < half, first, second) / half
    return x * lax.rsqrt(mean + epsilon) * gain


def finish_rows(arrived_ref, facts_ref, query_ref, row_ref):
    gains = facts_ref[facts_ref.shape[0] - 8 :]
    width = query_ref.shape[2]
    total, row = arrived_sum(arrived_ref, width, far_terms)
    lane = iota((8, 128), 1)
    query_gain, key_gain = gains[0:1], gains[1:2]
    for i in range(width // 128):
        at = slice(128 * i, 128 * (i + 1))
        part = normed(total[:, at], query_gain, lane, 64).astype(bf16)
        for k in range(query_ref.shape[0]):
            query_ref[k, :, at] = part
    row = jnp.where(iota((8, 128), 0) < 4, normed(row, key_gain, lane, 64), row)
    row_ref[...] = row.astype(bf16)


def stage(
    past_ref,
    accepted_ref,
    parents_ref,
    lambda_ref,
    query_gain_ref,
    key_gain_ref,
    head_gain_ref,
    keys_ref,
    values_ref,
    keys_vmem_ref,
    values_vmem_ref,
    keys_out_ref,
    values_out_ref,
    facts_ref,
    sems,
):
    taken = [
        pltpu.make_async_copy(keys_ref, keys_vmem_ref, sems.at[0]),
        pltpu.make_async_copy(values_ref, values_vmem_ref, sems.at[1]),
    ]
    put = [
        pltpu.make_async_copy(keys_vmem_ref, keys_out_ref, sems.at[2]),
        pltpu.make_async_copy(values_vmem_ref, values_out_ref, sems.at[3]),
    ]
    for c in taken:
        c.start()
    seqs, proposals = parents_ref.shape
    nears = lax.axis_size(near)
    far_index = lax.axis_index(far)
    own = near_place() * (seqs * proposals // nears) + far_index
    offset = (far_index * nears + near_place()) * (keys_ref.shape[1] // 4)
    own_seq, own_order = own // proposals, lax.rem(own, proposals)
    below = jnp.int32(0)
    for j in range(proposals):
        parent = parents_ref[own_seq, j]
        above = jnp.where(parent >= 0, (below >> jnp.maximum(parent, 0)) & 1, 0)
        below = below | (jnp.where(own_order == j, 1, above) << j)
    row = iota((rows, 128), 0)
    under = (below >> (2 * (row >> 4) + ((row >> 2) & 1))) & 1
    limit = jnp.zeros((8, 128), jnp.int32)
    for s in range(seqs):
        limit = jnp.where(iota((8, 128), 0) == s, past_ref[s] + accepted_ref[s] - offset, limit)
        facts_ref[rows * s : rows * (s + 1)] = jnp.where(own_seq == s, under, 0).astype(f32)
    scale = jnp.ones((rows, 128), f32)
    for h in range(4):
        scale = jnp.where(((row & 3) == h) & (((row >> 3) & 1) == 1), lambda_ref[h], scale)
    facts_ref[rows * seqs : rows * (seqs + 1)] = scale
    last = rows * (seqs + 1)
    facts_ref[last : last + 8] = limit.astype(f32)
    gains = [jnp.concatenate([ref[...]] * 2, axis=1) for ref in (query_gain_ref, key_gain_ref)]
    gains += [head_gain_ref[...], jnp.zeros((5, 128), f32)]
    facts_ref[last + 8 :] = jnp.concatenate(gains, axis=0)
    for c, d in zip(taken, put):
        c.wait()
        d.start()
    for d in put:
        d.wait()


def attend(
    facts_ref,
    query_ref,
    row_ref,
    keys_ref,
    values_ref,
    out_ref,
):
    seqs, columns = keys_ref.shape[:2]
    proposals = query_ref.shape[0] // seqs
    row = iota((rows, 128), 0)
    lane = iota((rows, 128), 1)
    row_head, row_comp = row & 3, (row >> 3) & 1
    row_order = 2 * (row >> 4) + ((row >> 2) & 1)
    spread = (iota((rows, proposals), 1) == row_order[:, :proposals]).astype(bf16)
    head_at = [row_head == h for h in range(4)]
    comp_at = (lane >= 64) == (row_comp == 1)
    column = iota((rows, columns), 1)
    same_head = (column & 3) == (iota((rows, columns), 0) & 3)
    position = jnp.where(same_head, (column >> 2).astype(f32), float(columns))
    scale = facts_ref[rows * seqs : rows * (seqs + 1)]
    last = rows * (seqs + 1)
    limits = facts_ref[last : last + 8]
    new_row = row_ref[...].astype(f32)
    new_key = jnp.concatenate([new_row[:4]] * (rows // 4), axis=0)
    new_value = jnp.concatenate([new_row[4:]] * (rows // 4), axis=0)
    for s in range(seqs):
        wide = jnp.dot(
            spread, query_ref[s * proposals : (s + 1) * proposals, :], preferred_element_type=f32
        )
        query = jnp.zeros((rows, 128), f32)
        for h in range(4):
            query = jnp.where(head_at[h], wide[:, 128 * h : 128 * (h + 1)], query)
        query = jnp.where(comp_at, query, 0.0)
        scores = lax.dot_general(
            query.astype(bf16),
            keys_ref[s],
            (((1,), (1,)), ((), ())),
            preferred_element_type=f32,
        )
        visible = position < jnp.minimum(limits[s : s + 1, :1], float(columns))
        masked = jnp.where(visible, scores * 0.125, floor_value)
        tree_score = jnp.sum(query * new_key, axis=-1, keepdims=True) * 0.125
        tree_visible = facts_ref[rows * s : rows * (s + 1), :1] > 0.5
        tree_masked = jnp.where(tree_visible, tree_score, floor_value)
        top = jnp.maximum(jnp.max(masked, axis=-1, keepdims=True), tree_masked)
        weights = jnp.where(visible, jnp.exp(masked - top), 0.0)
        tree_weight = jnp.where(tree_visible, jnp.exp(tree_masked - top), 0.0)
        total = jnp.sum(weights, axis=-1, keepdims=True) + tree_weight
        acc = jnp.dot(weights.astype(bf16), values_ref[s], preferred_element_type=f32)
        acc = (acc + tree_weight.astype(bf16).astype(f32) * new_value) * scale
        acc = acc.astype(bf16)
        stats = jnp.zeros((rows, 128), f32)
        for k, part in enumerate((*parts_of(top), *parts_of(total))):
            stats = jnp.where(lane == k, part, stats)
        stats = jnp.transpose(stats)[:8].astype(bf16)
        for r in range(out_ref.shape[0]):
            out_ref[r, s, :16, :] = acc[16 * r : 16 * (r + 1)]
            out_ref[r, s, 16:, :] = stats


def stat_rows(stats):
    return stats[0:1] + stats[1:2] + stats[2:3], stats[3:4] + stats[4:5] + stats[5:6]


def combine_near(arrived_ref, row_ref, out_ref, factor_ref):
    me = near_place()
    sources, groups = arrived_ref.shape[:2]
    tiles, factors = [], []
    lane = iota((8, 128), 1)
    packed = jnp.zeros((8, 128), f32)
    for g in range(groups):
        tops, sums = zip(*[stat_rows(arrived_ref[r, g, 16:, :].astype(f32)) for r in range(sources)])
        top = functools.reduce(jnp.maximum, tops)
        scales = [jnp.exp(t - top) for t in tops]
        total = sum(s * f for s, f in zip(sums, scales))
        factors.extend(scales)
        zero = jnp.zeros((1, 128), f32)
        stats = jnp.concatenate([*parts_of(top), *parts_of(total), zero, zero], axis=0)
        moved = pltpu.roll(stats, lax.rem(128 + 16 * g - 16 * me, 128), 1)
        packed = jnp.where((lane >> 4) == g, moved, packed)
    count = sources * groups
    wide = jnp.concatenate(factors + [jnp.zeros((128 - count, 128), f32)], axis=0)
    factor_ref[...] = jnp.transpose(wide)
    mine = factor_ref[pl.ds(pl.multiple_of(16 * me, 16), 16), :]
    for g in range(groups):
        acc = jnp.zeros((16, 128), f32)
        for r in range(sources):
            at = g * sources + r
            acc = acc + arrived_ref[r, g, :16, :].astype(f32) * mine[:, at : at + 1]
        tiles.append(acc.astype(bf16))
    for k in range(out_ref.shape[0]):
        for g in range(groups):
            out_ref[k, 16 * g : 16 * (g + 1), :] = tiles[g]
        out_ref[k, 64:72, :] = packed.astype(bf16)
        out_ref[k, 72:80, :] = row_ref[...]


def combine_far(arrived_ref, gain_ref, out_ref):
    sources = arrived_ref.shape[0]
    tops, sums = zip(*[stat_rows(arrived_ref[q, 64:72, :].astype(f32)) for q in range(sources)])
    top = functools.reduce(jnp.maximum, tops)
    scales = [jnp.exp(t - top) for t in tops]
    total = sum(s * f for s, f in zip(sums, scales))
    wide = jnp.concatenate(scales + [total, jnp.zeros((127 - sources, 128), f32)], axis=0)
    columns = jnp.transpose(wide)[:64]
    acc = jnp.zeros((64, 128), f32)
    for q in range(sources):
        acc = acc + arrived_ref[q, :64, :].astype(f32) * columns[:, q : q + 1]
    acc = acc / columns[:, sources : sources + 1]
    heads = []
    for g in range(4):
        mixture = acc[16 * g : 16 * g + 8] - acc[16 * g + 8 : 16 * g + 16]
        mean = jnp.mean(mixture * mixture, axis=-1, keepdims=True)
        heads.append((mixture * lax.rsqrt(mean + epsilon) * gain_ref[...]).astype(bf16))
    for k in range(out_ref.shape[0]):
        for g in range(4):
            out_ref[k, 8 * g : 8 * (g + 1), :] = heads[g]
        for q in range(sources):
            out_ref[k, 32 + 8 * q : 40 + 8 * q, :] = arrived_ref[q, 72:80, :]


def finish(
    past_ref,
    accepted_ref,
    arrived_ref,
    own_ref,
    first_ref,
    second_ref,
    third_ref,
    keys_ref,
    values_ref,
    out_ref,
    keys_out_ref,
    values_out_ref,
    heads_ref,
    key_rows,
    value_rows,
    lengths,
    sem,
):
    known = [
        pltpu.make_async_copy(past_ref, lengths.at[0], sem.at[0]),
        pltpu.make_async_copy(accepted_ref, lengths.at[1], sem.at[1]),
    ]
    for c in known:
        c.start()
    del keys_ref, values_ref
    sources = arrived_ref.shape[0]
    heads = jnp.concatenate([arrived_ref[r, :32, :] for r in range(sources)], axis=0)
    count = heads.shape[0]
    to = iota((count, count), 0)
    source = ((to >> 1) & 7) * 32 + (to >> 6) * 8 + (to & 1) * 4 + ((to >> 4) & 3)
    order = (iota((count, count), 1) == source).astype(bf16)
    heads_ref[...] = jnp.dot(order, heads, preferred_element_type=f32)
    total = jnp.zeros(out_ref.shape, f32)
    for k, weight_ref in enumerate((own_ref, first_ref, second_ref, third_ref)):
        g = lax.rem(lax.axis_index(tp) + 4 - k, 4)
        mine = heads_ref[pl.ds(pl.multiple_of(64 * g, 64), 64), :].astype(bf16)
        left = jnp.concatenate([mine[16 * h : 16 * (h + 1)] for h in range(4)], axis=1)
        group = lax.dot_general(
            left, weight_ref[...], (((1,), (1,)), ((), ())), preferred_element_type=f32
        )
        total = total + group.astype(bf16).astype(f32)
    out_ref[...] = total.astype(bf16)
    for c in known:
        c.wait()
    seqs, positions_dev = keys_out_ref.shape[:2]
    offset = (lax.axis_index(far) * lax.axis_size(near) + near_place()) * positions_dev
    proposals = key_rows.shape[0]
    for s in range(seqs):
        first = lengths[0, s] + lengths[1, s] - offset

        @pl.when((first > -proposals) & (first < positions_dev))
        def _():
            for j in range(proposals):
                r, q = divmod(s * proposals + j, sources)
                key_rows[j] = arrived_ref[r, 32 + 8 * q : 36 + 8 * q, :]
                value_rows[j] = arrived_ref[r, 36 + 8 * q : 40 + 8 * q, :]
            for j in range(proposals):

                @pl.when((first + j >= 0) & (first + j < positions_dev))
                def _():
                    at = jnp.clip(first + j, 0, positions_dev - 1)
                    writes = [
                        pltpu.make_async_copy(rows.at[j], whole.at[s, at], sem.at[k])
                        for k, (rows, whole) in enumerate(
                            ((key_rows, keys_out_ref), (value_rows, values_out_ref))
                        )
                    ]
                    for c in writes:
                        c.start()
                    for c in writes:
                        c.wait()


def on_device(
    hidden_states,
    w_query,
    w_key,
    w_value,
    query_gain,
    key_gain,
    lambda_head,
    head_gain,
    w_output,
    cache_keys,
    cache_values,
    past_lengths,
    accepted,
    parents,
):
    shape = jax.ShapeDtypeStruct
    seqs, proposals = parents.shape
    tokens = hidden_states.shape[0]
    width = w_query.shape[1]
    positions_dev, heads = cache_keys.shape[1:3]
    nears, fars, tps = (math.prod(lax.axis_size(a) for a in axes) for axes in (near, (far,), (tp,)))
    chunk = tokens // nears
    terms = call(
        project,
        shape((tokens, (near_terms + 2) * width), bf16),
        [hbm] * 4,
        room=65182 / 1024,
        scratch_shapes=[
            pltpu.VMEM(hidden_states.shape, bf16),
            pltpu.VMEM((3, *w_query.shape), bf16),
            pltpu.SemaphoreType.DMA((4,)),
        ],
    )(hidden_states, w_query, w_key, w_value)
    terms = lax.all_to_all(
        terms.reshape(nears, chunk, -1), near, 0, 0, tiled=True
    )
    shared = call(
        functools.partial(sum_near, width=width),
        shape((fars, chunk, far_terms * width + 128), bf16),
        [vmem],
    )(terms)
    shared = lax.all_to_all(shared, far, 0, 0, tiled=True)
    flat = (seqs, positions_dev * heads, 128)
    keys, values, keys_copy, values_copy, facts = call(
        stage,
        (
            *[shape(flat, bf16)] * 4,
            shape((rows * (seqs + 1) + 16, 128), f32),
        ),
        [smem] * 4 + [vmem] * 3 + [hbm] * 2,
        (vmem, vmem, hbm, hbm, vmem),
        scratch_shapes=[pltpu.SemaphoreType.DMA((4,))],
    )(
        past_lengths,
        accepted,
        parents,
        lambda_head,
        query_gain[None],
        key_gain[None],
        head_gain[None],
        cache_keys.reshape(flat),
        cache_values.reshape(flat),
    )
    query, row = call(
        finish_rows,
        (shape((nears, chunk, width), bf16), shape((8, 128), bf16)),
        [vmem] * 2,
        (vmem, vmem),
    )(shared, facts)
    query = lax.all_to_all(query, near, 0, 0, tiled=True).reshape(tokens, width)
    part = call(
        attend, shape((nears, tps, 24, 128), bf16), [vmem] * 5, flops=10000000, room=16
    )(facts, query, row, keys, values)
    part = lax.all_to_all(
        part.reshape(nears * tps, 24, 128), (*near, tp), 0, 0, tiled=True
    )
    part = call(
        combine_near,
        shape((fars, 80, 128), bf16),
        [vmem, vmem],
        scratch_shapes=[pltpu.VMEM((128, 128), f32)],
    )(part.reshape(nears, tps, 24, 128), row)
    part = lax.all_to_all(part, far, 0, 0, tiled=True)
    mixed = call(combine_far, shape((nears, 96, 128), bf16), [vmem] * 2)(part, head_gain[None])
    mixed = lax.all_to_all(mixed, near, 0, 0, tiled=True)
    own = w_output.T
    weights = [own]
    for k in range(1, tps):
        ring = [(i, (i + k) % tps) for i in range(tps)]
        weights.append(lax.ppermute(own, tp, ring))
    whole = cache_keys.shape
    return call(
        finish,
        (
            shape((proposals, w_output.shape[1]), bf16),
            shape(whole, bf16),
            shape(whole, bf16),
        ),
        [hbm] * 2 + [vmem] * 5 + [hbm] * 2,
        (vmem, hbm, hbm),
        scratch_shapes=[
            pltpu.VMEM((256, 128), f32),
            pltpu.VMEM((proposals, heads, 128), bf16),
            pltpu.VMEM((proposals, heads, 128), bf16),
            pltpu.SMEM((2, seqs), jnp.int32),
            pltpu.SemaphoreType.DMA((2,)),
        ],
        input_output_aliases={7: 1, 8: 2},
    )(past_lengths, accepted, mixed, *weights, keys_copy.reshape(whole), values_copy.reshape(whole))


def solution(mesh):
    groups, shards, tps = (mesh.shape[a] for a in ("grp", "kv", "tp"))
    split = (groups, shards // (near_chips * near_cores), near_chips, near_cores, tps)
    finer = Mesh(mesh.devices.reshape(split), ("grp", far, chip, core, tp))
    kv = (far, chip, core)
    cache = P("grp", kv, tp, None)
    placed = (
        P("grp", kv),
        P(kv, tp),
        P(kv, tp),
        P(kv, tp),
        P(),
        P(),
        P(tp),
        P(),
        P(tp, kv),
        cache,
        cache,
        P("grp"),
        P("grp"),
        P("grp", None),
    )
    return jax.shard_map(
        on_device,
        mesh=finer,
        in_specs=placed,
        out_specs=(P(("grp", tp), kv), cache, cache),
        check_vma=False,
    )
```

```python
import functools
import math

import jax
import jax.numpy as jnp
from jax import lax
from jax.experimental import pallas as pl
from jax.experimental.pallas import tpu as pltpu
from jax.sharding import Mesh
from jax.sharding import PartitionSpec as P


epsilon = 1e-06
floor_value = -1e30
f32 = jnp.float32
bf16 = jnp.bfloat16
interpreted = False
near_chips = 4
near_cores = 2
far, chip, core, tp = "far", "chip", "core", "tp"
near = (chip, core)
near_terms = 2
far_terms = 2
rows = 128

vmem = pl.BlockSpec(memory_space=pltpu.VMEM)
smem = pl.BlockSpec(memory_space=pltpu.SMEM)
hbm = pl.BlockSpec(memory_space=pltpu.HBM)


def near_place():
    return lax.axis_index(chip) * lax.axis_size(core) + lax.axis_index(core)


def iota(shape, dim):
    return lax.broadcasted_iota(jnp.int32, shape, dim)


def call(body, out_shape, in_specs, out_specs=vmem, flops=1000000, room=4, **rest):
    return pl.pallas_call(
        body,
        out_shape=out_shape,
        in_specs=in_specs,
        out_specs=out_specs,
        interpret=interpreted,
        compiler_params=pltpu.CompilerParams(vmem_limit_bytes=int(room * 1024) << 10),
        cost_estimate=pl.CostEstimate(flops=flops, bytes_accessed=1000000, transcendentals=0),
        **rest,
    )


def terms_of(x, count):
    terms = []
    for _ in range(count):
        terms.append(x.astype(bf16))
        x = x - terms[-1].astype(f32)
    return terms


def parts_of(x):
    high = x.astype(bf16).astype(f32)
    middle = (x - high).astype(bf16).astype(f32)
    return high, middle, x - high - middle


def project(hidden_ref, query_ref, key_ref, value_ref, out_ref, hidden, weights, sems):
    width = query_ref.shape[1]
    copies = [pltpu.make_async_copy(hidden_ref, hidden, sems.at[3])]
    for k, ref in enumerate((query_ref, key_ref, value_ref)):
        copies.append(pltpu.make_async_copy(ref, weights.at[k], sems.at[k]))
    for c in copies:
        c.start()
    at = 0
    copies[0].wait()
    for k, count in enumerate((near_terms, 1, 1)):
        copies[k + 1].wait()
        sums = jnp.dot(hidden[...], weights[k], preferred_element_type=f32)
        for term in terms_of(sums, count):
            out_ref[:, at : at + width] = term
            at += width


def arrived_sum(arrived_ref, width, terms):
    total = arrived_ref[0].astype(f32)
    for k in range(1, arrived_ref.shape[0]):
        total = total + arrived_ref[k].astype(f32)
    query = total[:, :width]
    for k in range(1, terms):
        query = query + total[:, k * width : (k + 1) * width]
    return query, total[:, terms * width :]


def sum_near(arrived_ref, out_ref, *, width, order):
    query, rest = arrived_sum(arrived_ref, width, near_terms)
    terms = terms_of(query, far_terms)
    for k, to in enumerate(order):
        for i, term in enumerate(terms):
            out_ref[k, :, i * width : (i + 1) * width] = term
        row = [rest[to : to + 1, 128 * i : 128 * (i + 1)] for i in range(8)]
        out_ref[k, :, far_terms * width :] = jnp.concatenate(row, axis=0).astype(bf16)


def normed(x, gain, lane, half):
    squares = x * x
    first = jnp.sum(jnp.where(lane < half, squares, 0.0), axis=-1, keepdims=True)
    second = jnp.sum(jnp.where(lane < half, 0.0, squares), axis=-1, keepdims=True)
    mean = jnp.where(lane < half, first, second) / half
    return x * lax.rsqrt(mean + epsilon) * gain


def finish_rows(arrived_ref, facts_ref, query_ref, row_ref):
    gains = facts_ref[facts_ref.shape[0] - 8 :]
    width = query_ref.shape[2]
    total, row = arrived_sum(arrived_ref, width, far_terms)
    lane = iota((8, 128), 1)
    query_gain, key_gain = gains[0:1], gains[1:2]
    for i in range(width // 128):
        at = slice(128 * i, 128 * (i + 1))
        part = normed(total[:, at], query_gain, lane, 64).astype(bf16)
        for k in range(query_ref.shape[0]):
            query_ref[k, :, at] = part
    row = jnp.where(iota((8, 128), 0) < 4, normed(row, key_gain, lane, 64), row)
    row_ref[...] = row.astype(bf16)


def stage(
    past_ref,
    accepted_ref,
    parents_ref,
    lambda_ref,
    query_gain_ref,
    key_gain_ref,
    head_gain_ref,
    keys_ref,
    values_ref,
    keys_vmem_ref,
    values_vmem_ref,
    keys_out_ref,
    values_out_ref,
    facts_ref,
    sems,
):
    taken = [
        pltpu.make_async_copy(keys_ref, keys_vmem_ref, sems.at[0]),
        pltpu.make_async_copy(values_ref, values_vmem_ref, sems.at[1]),
    ]
    put = [
        pltpu.make_async_copy(keys_vmem_ref, keys_out_ref, sems.at[2]),
        pltpu.make_async_copy(values_vmem_ref, values_out_ref, sems.at[3]),
    ]
    for c in taken:
        c.start()
    seqs, proposals = parents_ref.shape
    nears = lax.axis_size(near)
    far_index = lax.axis_index(far)
    own = near_place() * (seqs * proposals // nears) + far_index
    offset = (far_index * nears + near_place()) * (keys_ref.shape[1] // 4)
    own_seq, own_order = own // proposals, lax.rem(own, proposals)
    below = jnp.int32(0)
    for j in range(proposals):
        parent = parents_ref[own_seq, j]
        above = jnp.where(parent >= 0, (below >> jnp.maximum(parent, 0)) & 1, 0)
        below = below | (jnp.where(own_order == j, 1, above) << j)
    row = iota((rows, 128), 0)
    under = (below >> (2 * (row >> 4) + ((row >> 2) & 1))) & 1
    limit = jnp.zeros((8, 128), jnp.int32)
    for s in range(seqs):
        limit = jnp.where(iota((8, 128), 0) == s, past_ref[s] + accepted_ref[s] - offset, limit)
        facts_ref[rows * s : rows * (s + 1)] = jnp.where(own_seq == s, under, 0).astype(f32)
    scale = jnp.ones((rows, 128), f32)
    for h in range(4):
        scale = jnp.where(((row & 3) == h) & (((row >> 3) & 1) == 1), lambda_ref[h], scale)
    facts_ref[rows * seqs : rows * (seqs + 1)] = scale
    last = rows * (seqs + 1)
    facts_ref[last : last + 8] = limit.astype(f32)
    gains = [jnp.concatenate([ref[...]] * 2, axis=1) for ref in (query_gain_ref, key_gain_ref)]
    gains += [head_gain_ref[...], jnp.zeros((5, 128), f32)]
    facts_ref[last + 8 :] = jnp.concatenate(gains, axis=0)
    for c, d in zip(taken, put):
        c.wait()
        d.start()
    for d in put:
        d.wait()


def attend(
    facts_ref,
    query_ref,
    row_ref,
    keys_ref,
    values_ref,
    out_ref,
):
    seqs, columns = keys_ref.shape[:2]
    proposals = query_ref.shape[0] // seqs
    row = iota((rows, 128), 0)
    lane = iota((rows, 128), 1)
    row_head, row_comp = row & 3, (row >> 3) & 1
    row_order = 2 * (row >> 4) + ((row >> 2) & 1)
    spread = (iota((rows, proposals), 1) == row_order[:, :proposals]).astype(bf16)
    head_at = [row_head == h for h in range(4)]
    comp_at = (lane >= 64) == (row_comp == 1)
    column = iota((rows, columns), 1)
    same_head = (column & 3) == (iota((rows, columns), 0) & 3)
    position = jnp.where(same_head, (column >> 2).astype(f32), float(columns))
    scale = facts_ref[rows * seqs : rows * (seqs + 1)]
    last = rows * (seqs + 1)
    limits = facts_ref[last : last + 8]
    new_row = row_ref[...].astype(f32)
    new_key = jnp.concatenate([new_row[:4]] * (rows // 4), axis=0)
    new_value = jnp.concatenate([new_row[4:]] * (rows // 4), axis=0)
    for s in range(seqs):
        wide = jnp.dot(
            spread, query_ref[s * proposals : (s + 1) * proposals, :], preferred_element_type=f32
        )
        query = jnp.zeros((rows, 128), f32)
        for h in range(4):
            query = jnp.where(head_at[h], wide[:, 128 * h : 128 * (h + 1)], query)
        query = jnp.where(comp_at, query, 0.0)
        scores = lax.dot_general(
            query.astype(bf16),
            keys_ref[s],
            (((1,), (1,)), ((), ())),
            preferred_element_type=f32,
        )
        visible = position < jnp.minimum(limits[s : s + 1, :1], float(columns))
        masked = jnp.where(visible, scores * 0.125, floor_value)
        tree_score = jnp.sum(query * new_key, axis=-1, keepdims=True) * 0.125
        tree_visible = facts_ref[rows * s : rows * (s + 1), :1] > 0.5
        tree_masked = jnp.where(tree_visible, tree_score, floor_value)
        top = jnp.maximum(jnp.max(masked, axis=-1, keepdims=True), tree_masked)
        weights = jnp.where(visible, jnp.exp(masked - top), 0.0)
        tree_weight = jnp.where(tree_visible, jnp.exp(tree_masked - top), 0.0)
        total = jnp.sum(weights, axis=-1, keepdims=True) + tree_weight
        acc = jnp.dot(weights.astype(bf16), values_ref[s], preferred_element_type=f32)
        acc = (acc + tree_weight.astype(bf16).astype(f32) * new_value) * scale
        acc = acc.astype(bf16)
        stats = jnp.zeros((rows, 128), f32)
        for k, part in enumerate((*parts_of(top), *parts_of(total))):
            stats = jnp.where(lane == k, part, stats)
        stats = jnp.transpose(stats)[:8].astype(bf16)
        for r in range(out_ref.shape[0]):
            out_ref[r, s, :16, :] = acc[16 * r : 16 * (r + 1)]
            out_ref[r, s, 16:, :] = stats


def stat_rows(stats):
    return stats[0:1] + stats[1:2] + stats[2:3], stats[3:4] + stats[4:5] + stats[5:6]


def combine_near(arrived_ref, row_ref, out_ref, factor_ref):
    me = near_place()
    sources, groups = arrived_ref.shape[:2]
    tiles, factors = [], []
    lane = iota((8, 128), 1)
    packed = jnp.zeros((8, 128), f32)
    for g in range(groups):
        tops, sums = zip(*[stat_rows(arrived_ref[r, g, 16:, :].astype(f32)) for r in range(sources)])
        top = functools.reduce(jnp.maximum, tops)
        scales = [jnp.exp(t - top) for t in tops]
        total = sum(s * f for s, f in zip(sums, scales))
        factors.extend(scales)
        zero = jnp.zeros((1, 128), f32)
        stats = jnp.concatenate([*parts_of(top), *parts_of(total), zero, zero], axis=0)
        moved = pltpu.roll(stats, lax.rem(128 + 16 * g - 16 * me, 128), 1)
        packed = jnp.where((lane >> 4) == g, moved, packed)
    count = sources * groups
    wide = jnp.concatenate(factors + [jnp.zeros((128 - count, 128), f32)], axis=0)
    factor_ref[...] = jnp.transpose(wide)
    mine = factor_ref[pl.ds(pl.multiple_of(16 * me, 16), 16), :]
    for g in range(groups):
        acc = jnp.zeros((16, 128), f32)
        for r in range(sources):
            at = g * sources + r
            acc = acc + arrived_ref[r, g, :16, :].astype(f32) * mine[:, at : at + 1]
        tiles.append(acc.astype(bf16))
    for k in range(out_ref.shape[0]):
        for g in range(groups):
            out_ref[k, 16 * g : 16 * (g + 1), :] = tiles[g]
        out_ref[k, 64:72, :] = packed.astype(bf16)
        out_ref[k, 72:80, :] = row_ref[...]


def combine_far(arrived_ref, gain_ref, out_ref, *, order):
    sources = arrived_ref.shape[0]
    tops, sums = zip(*[stat_rows(arrived_ref[q, 64:72, :].astype(f32)) for q in range(sources)])
    top = functools.reduce(jnp.maximum, tops)
    scales = [jnp.exp(t - top) for t in tops]
    total = sum(s * f for s, f in zip(sums, scales))
    wide = jnp.concatenate(scales + [total, jnp.zeros((127 - sources, 128), f32)], axis=0)
    columns = jnp.transpose(wide)[:64]
    acc = jnp.zeros((64, 128), f32)
    for q in range(sources):
        acc = acc + arrived_ref[q, :64, :].astype(f32) * columns[:, q : q + 1]
    acc = acc / columns[:, sources : sources + 1]
    heads = []
    for g in range(4):
        mixture = acc[16 * g : 16 * g + 8] - acc[16 * g + 8 : 16 * g + 16]
        mean = jnp.mean(mixture * mixture, axis=-1, keepdims=True)
        heads.append((mixture * lax.rsqrt(mean + epsilon) * gain_ref[...]).astype(bf16))
    for k in range(out_ref.shape[0]):
        for g in range(4):
            out_ref[k, 8 * g : 8 * (g + 1), :] = heads[g]
        for q, source in enumerate(order):
            at = 32 + 8 * source
            out_ref[k, at : at + 8, :] = arrived_ref[q, 72:80, :]


def finish(
    past_ref,
    accepted_ref,
    arrived_ref,
    own_ref,
    first_ref,
    second_ref,
    third_ref,
    keys_ref,
    values_ref,
    out_ref,
    keys_out_ref,
    values_out_ref,
    heads_ref,
    key_rows,
    value_rows,
    lengths,
    sem,
):
    known = [
        pltpu.make_async_copy(past_ref, lengths.at[0], sem.at[0]),
        pltpu.make_async_copy(accepted_ref, lengths.at[1], sem.at[1]),
    ]
    for c in known:
        c.start()
    del keys_ref, values_ref
    sources = arrived_ref.shape[0]
    heads = jnp.concatenate([arrived_ref[r, :32, :] for r in range(sources)], axis=0)
    count = heads.shape[0]
    to = iota((count, count), 0)
    source = ((to >> 1) & 7) * 32 + (to >> 6) * 8 + (to & 1) * 4 + ((to >> 4) & 3)
    order = (iota((count, count), 1) == source).astype(bf16)
    heads_ref[...] = jnp.dot(order, heads, preferred_element_type=f32)
    total = jnp.zeros(out_ref.shape, f32)
    for k, weight_ref in enumerate((own_ref, first_ref, second_ref, third_ref)):
        g = lax.rem(lax.axis_index(tp) + 4 - k, 4)
        mine = heads_ref[pl.ds(pl.multiple_of(64 * g, 64), 64), :].astype(bf16)
        left = jnp.concatenate([mine[16 * h : 16 * (h + 1)] for h in range(4)], axis=1)
        group = lax.dot_general(
            left, weight_ref[...], (((1,), (1,)), ((), ())), preferred_element_type=f32
        )
        total = total + group.astype(bf16).astype(f32)
    out_ref[...] = total.astype(bf16)
    for c in known:
        c.wait()
    seqs, positions_dev = keys_out_ref.shape[:2]
    offset = (lax.axis_index(far) * lax.axis_size(near) + near_place()) * positions_dev
    proposals = key_rows.shape[0]
    for s in range(seqs):
        first = lengths[0, s] + lengths[1, s] - offset

        @pl.when((first > -proposals) & (first < positions_dev))
        def _():
            for j in range(proposals):
                r, q = divmod(s * proposals + j, sources)
                key_rows[j] = arrived_ref[r, 32 + 8 * q : 36 + 8 * q, :]
                value_rows[j] = arrived_ref[r, 36 + 8 * q : 40 + 8 * q, :]
            for j in range(proposals):

                @pl.when((first + j >= 0) & (first + j < positions_dev))
                def _():
                    at = jnp.clip(first + j, 0, positions_dev - 1)
                    writes = [
                        pltpu.make_async_copy(rows.at[j], whole.at[s, at], sem.at[k])
                        for k, (rows, whole) in enumerate(
                            ((key_rows, keys_out_ref), (value_rows, values_out_ref))
                        )
                    ]
                    for c in writes:
                        c.start()
                    for c in writes:
                        c.wait()


def on_device(
    hidden_states,
    w_query,
    w_key,
    w_value,
    query_gain,
    key_gain,
    lambda_head,
    head_gain,
    w_output,
    cache_keys,
    cache_values,
    past_lengths,
    accepted,
    parents,
):
    shape = jax.ShapeDtypeStruct
    seqs, proposals = parents.shape
    tokens = hidden_states.shape[0]
    width = w_query.shape[1]
    positions_dev, heads = cache_keys.shape[1:3]
    nears, fars, tps = (math.prod(lax.axis_size(a) for a in axes) for axes in (near, (far,), (tp,)))
    chunk = tokens // nears
    apart = [min(b + 1, fars - 1 - b) for b in range(fars)]
    first_order = sorted(range(fars), key=lambda b: -apart[b])
    second_order = list(reversed(range(fars)))
    terms = call(
        project,
        shape((tokens, (near_terms + 2) * width), bf16),
        [hbm] * 4,
        room=65182 / 1024,
        scratch_shapes=[
            pltpu.VMEM(hidden_states.shape, bf16),
            pltpu.VMEM((3, *w_query.shape), bf16),
            pltpu.SemaphoreType.DMA((4,)),
        ],
    )(hidden_states, w_query, w_key, w_value)
    terms = lax.all_to_all(
        terms.reshape(nears, chunk, -1), near, 0, 0, tiled=True
    )
    shared = call(
        functools.partial(sum_near, width=width, order=first_order),
        shape((fars, chunk, far_terms * width + 128), bf16),
        [vmem],
    )(terms)
    shared = lax.all_to_all(
        shared, far, 0, 0, tiled=True, axis_index_groups=[first_order]
    )
    flat = (seqs, positions_dev * heads, 128)
    keys, values, keys_copy, values_copy, facts = call(
        stage,
        (
            *[shape(flat, bf16)] * 4,
            shape((rows * (seqs + 1) + 16, 128), f32),
        ),
        [smem] * 4 + [vmem] * 3 + [hbm] * 2,
        (vmem, vmem, hbm, hbm, vmem),
        scratch_shapes=[pltpu.SemaphoreType.DMA((4,))],
    )(
        past_lengths,
        accepted,
        parents,
        lambda_head,
        query_gain[None],
        key_gain[None],
        head_gain[None],
        cache_keys.reshape(flat),
        cache_values.reshape(flat),
    )
    query, row = call(
        finish_rows,
        (shape((nears, chunk, width), bf16), shape((8, 128), bf16)),
        [vmem] * 2,
        (vmem, vmem),
    )(shared, facts)
    query = lax.all_to_all(query, near, 0, 0, tiled=True).reshape(tokens, width)
    part = call(
        attend, shape((nears, tps, 24, 128), bf16), [vmem] * 5, flops=10000000, room=16
    )(facts, query, row, keys, values)
    part = lax.all_to_all(
        part.reshape(nears * tps, 24, 128), (*near, tp), 0, 0, tiled=True
    )
    part = call(
        combine_near,
        shape((fars, 80, 128), bf16),
        [vmem, vmem],
        scratch_shapes=[pltpu.VMEM((128, 128), f32)],
    )(part.reshape(nears, tps, 24, 128), row)
    part = lax.all_to_all(
        part, far, 0, 0, tiled=True, axis_index_groups=[second_order]
    )
    mixed = call(
        functools.partial(combine_far, order=second_order),
        shape((nears, 96, 128), bf16),
        [vmem] * 2,
    )(part, head_gain[None])
    mixed = lax.all_to_all(mixed, near, 0, 0, tiled=True)
    own = w_output.T
    weights = [own]
    for k in range(1, tps):
        ring = [(i, (i + k) % tps) for i in range(tps)]
        weights.append(lax.ppermute(own, tp, ring))
    whole = cache_keys.shape
    return call(
        finish,
        (
            shape((proposals, w_output.shape[1]), bf16),
            shape(whole, bf16),
            shape(whole, bf16),
        ),
        [hbm] * 2 + [vmem] * 5 + [hbm] * 2,
        (vmem, hbm, hbm),
        scratch_shapes=[
            pltpu.VMEM((256, 128), f32),
            pltpu.VMEM((proposals, heads, 128), bf16),
            pltpu.VMEM((proposals, heads, 128), bf16),
            pltpu.SMEM((2, seqs), jnp.int32),
            pltpu.SemaphoreType.DMA((2,)),
        ],
        input_output_aliases={7: 1, 8: 2},
    )(past_lengths, accepted, mixed, *weights, keys_copy.reshape(whole), values_copy.reshape(whole))


def solution(mesh):
    groups, shards, tps = (mesh.shape[a] for a in ("grp", "kv", "tp"))
    split = (groups, shards // (near_chips * near_cores), near_chips, near_cores, tps)
    finer = Mesh(mesh.devices.reshape(split), ("grp", far, chip, core, tp))
    kv = (far, chip, core)
    cache = P("grp", kv, tp, None)
    placed = (
        P("grp", kv),
        P(kv, tp),
        P(kv, tp),
        P(kv, tp),
        P(),
        P(),
        P(tp),
        P(),
        P(tp, kv),
        cache,
        cache,
        P("grp"),
        P("grp"),
        P("grp", None),
    )
    return jax.shard_map(
        on_device,
        mesh=finer,
        in_specs=placed,
        out_specs=(P(("grp", tp), kv), cache, cache),
        check_vma=False,
    )
```

```python
import functools
import math

import jax
import jax.numpy as jnp
from jax import lax
from jax.experimental import pallas as pl
from jax.experimental.pallas import tpu as pltpu
from jax.sharding import Mesh
from jax.sharding import PartitionSpec as P


epsilon = 1e-06
floor_value = -1e30
f32 = jnp.float32
bf16 = jnp.bfloat16
interpreted = False
near_chips = 4
near_cores = 2
far, chip, core, tp = "far", "chip", "core", "tp"
near = (chip, core)
near_terms = 2
far_terms = 2
rows = 128

vmem = pl.BlockSpec(memory_space=pltpu.VMEM)
smem = pl.BlockSpec(memory_space=pltpu.SMEM)
hbm = pl.BlockSpec(memory_space=pltpu.HBM)


def near_place():
    return lax.axis_index(chip) * lax.axis_size(core) + lax.axis_index(core)


def iota(shape, dim):
    return lax.broadcasted_iota(jnp.int32, shape, dim)


def call(body, out_shape, in_specs, out_specs=vmem, flops=1000000, room=4, **rest):
    return pl.pallas_call(
        body,
        out_shape=out_shape,
        in_specs=in_specs,
        out_specs=out_specs,
        interpret=interpreted,
        compiler_params=pltpu.CompilerParams(vmem_limit_bytes=int(room * 1024) << 10),
        cost_estimate=pl.CostEstimate(flops=flops, bytes_accessed=1000000, transcendentals=0),
        **rest,
    )


def terms_of(x, count):
    terms = []
    for _ in range(count):
        terms.append(x.astype(bf16))
        x = x - terms[-1].astype(f32)
    return terms


def parts_of(x):
    high = x.astype(bf16).astype(f32)
    middle = (x - high).astype(bf16).astype(f32)
    return high, middle, x - high - middle


def project(hidden_ref, query_ref, key_ref, value_ref, out_ref, hidden, weights, sems):
    width = query_ref.shape[1]
    copies = [pltpu.make_async_copy(hidden_ref, hidden, sems.at[3])]
    for k, ref in enumerate((query_ref, key_ref, value_ref)):
        copies.append(pltpu.make_async_copy(ref, weights.at[k], sems.at[k]))
    for c in copies:
        c.start()
    at = 0
    copies[0].wait()
    for k, count in enumerate((near_terms, 1, 1)):
        copies[k + 1].wait()
        sums = jnp.dot(hidden[...], weights[k], preferred_element_type=f32)
        for term in terms_of(sums, count):
            out_ref[:, at : at + width] = term
            at += width


def arrived_sum(arrived_ref, width, terms):
    total = arrived_ref[0].astype(f32)
    for k in range(1, arrived_ref.shape[0]):
        total = total + arrived_ref[k].astype(f32)
    query = total[:, :width]
    for k in range(1, terms):
        query = query + total[:, k * width : (k + 1) * width]
    return query, total[:, terms * width :]


def sum_near(arrived_ref, out_ref, *, width):
    query, rest = arrived_sum(arrived_ref, width, near_terms)
    terms = terms_of(query, far_terms)
    for k in range(out_ref.shape[0]):
        for i, term in enumerate(terms):
            out_ref[k, :, i * width : (i + 1) * width] = term
        row = [rest[k : k + 1, 128 * i : 128 * (i + 1)] for i in range(8)]
        out_ref[k, :, far_terms * width :] = jnp.concatenate(row, axis=0).astype(bf16)


def normed(x, gain, lane, half):
    squares = x * x
    first = jnp.sum(jnp.where(lane < half, squares, 0.0), axis=-1, keepdims=True)
    second = jnp.sum(jnp.where(lane < half, 0.0, squares), axis=-1, keepdims=True)
    mean = jnp.where(lane < half, first, second) / half
    return x * lax.rsqrt(mean + epsilon) * gain


def finish_rows(arrived_ref, facts_ref, query_ref, row_ref):
    gains = facts_ref[facts_ref.shape[0] - 8 :]
    width = query_ref.shape[2]
    total, row = arrived_sum(arrived_ref, width, far_terms)
    lane = iota((8, 128), 1)
    query_gain, key_gain = gains[0:1], gains[1:2]
    for i in range(width // 128):
        at = slice(128 * i, 128 * (i + 1))
        part = normed(total[:, at], query_gain, lane, 64).astype(bf16)
        for k in range(query_ref.shape[0]):
            query_ref[k, :, at] = part
    row = jnp.where(iota((8, 128), 0) < 4, normed(row, key_gain, lane, 64), row)
    row_ref[...] = row.astype(bf16)


def stage(
    past_ref,
    accepted_ref,
    parents_ref,
    lambda_ref,
    query_gain_ref,
    key_gain_ref,
    head_gain_ref,
    keys_ref,
    values_ref,
    keys_vmem_ref,
    values_vmem_ref,
    keys_out_ref,
    values_out_ref,
    facts_ref,
    raw,
    wide,
    sems,
):
    taken = [
        pltpu.make_async_copy(keys_ref, raw.at[0], sems.at[0]),
        pltpu.make_async_copy(values_ref, raw.at[1], sems.at[1]),
    ]
    put = [
        pltpu.make_async_copy(raw.at[0], keys_out_ref, sems.at[2]),
        pltpu.make_async_copy(raw.at[1], values_out_ref, sems.at[3]),
    ]
    for c in taken:
        c.start()
    seqs, proposals = parents_ref.shape
    nears = lax.axis_size(near)
    far_index = lax.axis_index(far)
    own = near_place() * (seqs * proposals // nears) + far_index
    offset = (far_index * nears + near_place()) * (keys_ref.shape[1] // 4)
    own_seq, own_order = own // proposals, lax.rem(own, proposals)
    below = jnp.int32(0)
    for j in range(proposals):
        parent = parents_ref[own_seq, j]
        above = jnp.where(parent >= 0, (below >> jnp.maximum(parent, 0)) & 1, 0)
        below = below | (jnp.where(own_order == j, 1, above) << j)
    row = iota((rows, 128), 0)
    under = (below >> (2 * ((row >> 2) & 7) + (row & 1))) & 1
    limit = jnp.zeros((8, 128), jnp.int32)
    for s in range(seqs):
        limit = jnp.where(iota((8, 128), 0) == s, past_ref[s] + accepted_ref[s] - offset, limit)
        facts_ref[rows * s : rows * (s + 1)] = jnp.where(own_seq == s, under, 0).astype(f32)
    scale = jnp.ones((rows, 128), f32)
    for h in range(4):
        scale = jnp.where(((row >> 5) == h) & (((row >> 1) & 1) == 1), lambda_ref[h], scale)
    facts_ref[rows * seqs : rows * (seqs + 1)] = scale
    last = rows * (seqs + 1)
    facts_ref[last : last + 8] = limit.astype(f32)
    gains = [jnp.concatenate([ref[...]] * 2, axis=1) for ref in (query_gain_ref, key_gain_ref)]
    gains += [head_gain_ref[...], jnp.zeros((5, 128), f32)]
    facts_ref[last + 8 :] = jnp.concatenate(gains, axis=0)
    heads = keys_vmem_ref.shape[0] // seqs
    for k, out_ref in enumerate((keys_vmem_ref, values_vmem_ref)):
        taken[k].wait()
        put[k].start()
        for q in range(seqs):
            wide[...] = raw[k, q].astype(f32)
            for h in range(heads):
                part = wide[pl.ds(h, out_ref.shape[1], stride=heads), :]
                out_ref[q * heads + h] = part.astype(bf16)
    for d in put:
        d.wait()


def attend(
    facts_ref,
    query_ref,
    row_ref,
    keys_ref,
    values_ref,
    out_ref,
):
    seqs = out_ref.shape[1]
    heads = keys_ref.shape[0] // seqs
    positions_dev = keys_ref.shape[1]
    proposals = query_ref.shape[0] // seqs
    count = rows // heads
    line = iota((count, 128), 0)
    line_order = 2 * (line >> 2) + (line & 1)
    spread = (iota((count, proposals), 1) == line_order[:, :proposals]).astype(bf16)
    comp_at = (iota((count, 128), 1) >= 64) == (((line >> 1) & 1) == 1)
    row = iota((rows, rows), 0)
    lane = iota((rows, rows), 1)
    sent = (lane == count * (row & 3) + (row >> 2)).astype(bf16)
    last = rows * (seqs + 1)
    limits = facts_ref[last : last + 8]
    scale = facts_ref[rows * seqs : last]
    position = iota((count, positions_dev), 1).astype(f32)
    new_row = row_ref[...].astype(f32)
    for s in range(seqs):
        wide = jnp.dot(
            spread, query_ref[s * proposals : (s + 1) * proposals, :], preferred_element_type=f32
        )
        visible = position < jnp.minimum(limits[s : s + 1, :1], float(positions_dev))
        tree_visible = facts_ref[rows * s : rows * s + count, :1] > 0.5
        accs, tops, totals = [], [], []
        for h in range(heads):
            query = jnp.where(comp_at, wide[:, 128 * h : 128 * (h + 1)], 0.0)
            scores = lax.dot_general(
                query.astype(bf16),
                keys_ref[s * heads + h],
                (((1,), (1,)), ((), ())),
                preferred_element_type=f32,
            )
            masked = jnp.where(visible, scores * 0.125, floor_value)
            tree_score = jnp.sum(query * new_row[h : h + 1], axis=-1, keepdims=True) * 0.125
            tree_masked = jnp.where(tree_visible, tree_score, floor_value)
            top = jnp.maximum(jnp.max(masked, axis=-1, keepdims=True), tree_masked)
            weights = jnp.where(visible, jnp.exp(masked - top), 0.0)
            tree_weight = jnp.where(tree_visible, jnp.exp(tree_masked - top), 0.0)
            acc = jnp.dot(
                weights.astype(bf16), values_ref[s * heads + h], preferred_element_type=f32
            )
            value = new_row[heads + h : heads + h + 1]
            accs.append(acc + tree_weight.astype(bf16).astype(f32) * value)
            tops.append(top)
            totals.append(jnp.sum(weights, axis=-1, keepdims=True) + tree_weight)
        acc = jnp.concatenate(accs, axis=0) * scale
        top = jnp.concatenate(tops, axis=0)
        total = jnp.concatenate(totals, axis=0)
        stats = jnp.zeros((rows, 128), f32)
        for k, part in enumerate((*parts_of(top), *parts_of(total))):
            stats = jnp.where(lane == k, part, stats)
        both = jnp.concatenate([acc.astype(bf16), stats.astype(bf16)], axis=1)
        both = jnp.dot(sent, both, preferred_element_type=f32)
        acc = both[:, :128].astype(bf16)
        stats = jnp.transpose(both[:, 128:])[:8].astype(bf16)
        for r in range(out_ref.shape[0]):
            out_ref[r, s, :16, :] = acc[16 * r : 16 * (r + 1)]
            out_ref[r, s, 16:, :] = stats


def stat_rows(stats):
    return stats[0:1] + stats[1:2] + stats[2:3], stats[3:4] + stats[4:5] + stats[5:6]


def combine_near(arrived_ref, row_ref, out_ref, factor_ref):
    me = near_place()
    sources, groups = arrived_ref.shape[:2]
    tiles, factors = [], []
    lane = iota((8, 128), 1)
    packed = jnp.zeros((8, 128), f32)
    for g in range(groups):
        tops, sums = zip(*[stat_rows(arrived_ref[r, g, 16:, :].astype(f32)) for r in range(sources)])
        top = functools.reduce(jnp.maximum, tops)
        scales = [jnp.exp(t - top) for t in tops]
        total = sum(s * f for s, f in zip(sums, scales))
        factors.extend(scales)
        zero = jnp.zeros((1, 128), f32)
        stats = jnp.concatenate([*parts_of(top), *parts_of(total), zero, zero], axis=0)
        moved = pltpu.roll(stats, lax.rem(128 + 16 * g - 16 * me, 128), 1)
        packed = jnp.where((lane >> 4) == g, moved, packed)
    count = sources * groups
    wide = jnp.concatenate(factors + [jnp.zeros((128 - count, 128), f32)], axis=0)
    factor_ref[...] = jnp.transpose(wide)
    mine = factor_ref[pl.ds(pl.multiple_of(16 * me, 16), 16), :]
    for g in range(groups):
        acc = jnp.zeros((16, 128), f32)
        for r in range(sources):
            at = g * sources + r
            acc = acc + arrived_ref[r, g, :16, :].astype(f32) * mine[:, at : at + 1]
        tiles.append(acc.astype(bf16))
    for k in range(out_ref.shape[0]):
        for g in range(groups):
            out_ref[k, 16 * g : 16 * (g + 1), :] = tiles[g]
        out_ref[k, 64:72, :] = packed.astype(bf16)
        out_ref[k, 72:80, :] = row_ref[...]


def combine_far(arrived_ref, gain_ref, out_ref):
    sources = arrived_ref.shape[0]
    tops, sums = zip(*[stat_rows(arrived_ref[q, 64:72, :].astype(f32)) for q in range(sources)])
    top = functools.reduce(jnp.maximum, tops)
    scales = [jnp.exp(t - top) for t in tops]
    total = sum(s * f for s, f in zip(sums, scales))
    wide = jnp.concatenate(scales + [total, jnp.zeros((127 - sources, 128), f32)], axis=0)
    columns = jnp.transpose(wide)[:64]
    acc = jnp.zeros((64, 128), f32)
    for q in range(sources):
        acc = acc + arrived_ref[q, :64, :].astype(f32) * columns[:, q : q + 1]
    acc = acc / columns[:, sources : sources + 1]
    heads = []
    for g in range(4):
        mixture = acc[16 * g : 16 * g + 8] - acc[16 * g + 8 : 16 * g + 16]
        mean = jnp.mean(mixture * mixture, axis=-1, keepdims=True)
        heads.append((mixture * lax.rsqrt(mean + epsilon) * gain_ref[...]).astype(bf16))
    for k in range(out_ref.shape[0]):
        for g in range(4):
            out_ref[k, 8 * g : 8 * (g + 1), :] = heads[g]
        for q in range(sources):
            out_ref[k, 32 + 8 * q : 40 + 8 * q, :] = arrived_ref[q, 72:80, :]


def finish(
    past_ref,
    accepted_ref,
    arrived_ref,
    own_ref,
    first_ref,
    second_ref,
    third_ref,
    keys_ref,
    values_ref,
    out_ref,
    keys_out_ref,
    values_out_ref,
    heads_ref,
    key_rows,
    value_rows,
    lengths,
    sem,
):
    known = [
        pltpu.make_async_copy(past_ref, lengths.at[0], sem.at[0]),
        pltpu.make_async_copy(accepted_ref, lengths.at[1], sem.at[1]),
    ]
    for c in known:
        c.start()
    del keys_ref, values_ref
    sources = arrived_ref.shape[0]
    heads = jnp.concatenate([arrived_ref[r, :32, :] for r in range(sources)], axis=0)
    count = heads.shape[0]
    to = iota((count, count), 0)
    source = ((to >> 1) & 7) * 32 + (to >> 6) * 8 + (to & 1) * 4 + ((to >> 4) & 3)
    order = (iota((count, count), 1) == source).astype(bf16)
    heads_ref[...] = jnp.dot(order, heads, preferred_element_type=f32)
    total = jnp.zeros(out_ref.shape, f32)
    for k, weight_ref in enumerate((own_ref, first_ref, second_ref, third_ref)):
        g = lax.rem(lax.axis_index(tp) + 4 - k, 4)
        mine = heads_ref[pl.ds(pl.multiple_of(64 * g, 64), 64), :].astype(bf16)
        left = jnp.concatenate([mine[16 * h : 16 * (h + 1)] for h in range(4)], axis=1)
        group = lax.dot_general(
            left, weight_ref[...], (((1,), (1,)), ((), ())), preferred_element_type=f32
        )
        total = total + group.astype(bf16).astype(f32)
    out_ref[...] = total.astype(bf16)
    for c in known:
        c.wait()
    seqs, positions_dev = keys_out_ref.shape[:2]
    offset = (lax.axis_index(far) * lax.axis_size(near) + near_place()) * positions_dev
    proposals = key_rows.shape[0]
    for s in range(seqs):
        first = lengths[0, s] + lengths[1, s] - offset

        @pl.when((first > -proposals) & (first < positions_dev))
        def _():
            for j in range(proposals):
                r, q = divmod(s * proposals + j, sources)
                key_rows[j] = arrived_ref[r, 32 + 8 * q : 36 + 8 * q, :]
                value_rows[j] = arrived_ref[r, 36 + 8 * q : 40 + 8 * q, :]
            for j in range(proposals):

                @pl.when((first + j >= 0) & (first + j < positions_dev))
                def _():
                    at = jnp.clip(first + j, 0, positions_dev - 1)
                    writes = [
                        pltpu.make_async_copy(rows.at[j], whole.at[s, at], sem.at[k])
                        for k, (rows, whole) in enumerate(
                            ((key_rows, keys_out_ref), (value_rows, values_out_ref))
                        )
                    ]
                    for c in writes:
                        c.start()
                    for c in writes:
                        c.wait()


def on_device(
    hidden_states,
    w_query,
    w_key,
    w_value,
    query_gain,
    key_gain,
    lambda_head,
    head_gain,
    w_output,
    cache_keys,
    cache_values,
    past_lengths,
    accepted,
    parents,
):
    shape = jax.ShapeDtypeStruct
    seqs, proposals = parents.shape
    tokens = hidden_states.shape[0]
    width = w_query.shape[1]
    positions_dev, heads = cache_keys.shape[1:3]
    nears, fars, tps = (math.prod(lax.axis_size(a) for a in axes) for axes in (near, (far,), (tp,)))
    chunk = tokens // nears
    terms = call(
        project,
        shape((tokens, (near_terms + 2) * width), bf16),
        [hbm] * 4,
        room=65182 / 1024,
        scratch_shapes=[
            pltpu.VMEM(hidden_states.shape, bf16),
            pltpu.VMEM((3, *w_query.shape), bf16),
            pltpu.SemaphoreType.DMA((4,)),
        ],
    )(hidden_states, w_query, w_key, w_value)
    terms = lax.all_to_all(
        terms.reshape(nears, chunk, -1), near, 0, 0, tiled=True
    )
    shared = call(
        functools.partial(sum_near, width=width),
        shape((fars, chunk, far_terms * width + 128), bf16),
        [vmem],
    )(terms)
    shared = lax.all_to_all(shared, far, 0, 0, tiled=True)
    flat = (seqs, positions_dev * heads, 128)
    keys, values, keys_copy, values_copy, facts = call(
        stage,
        (
            *[shape((seqs * heads, positions_dev, 128), bf16)] * 2,
            *[shape(flat, bf16)] * 2,
            shape((rows * (seqs + 1) + 16, 128), f32),
        ),
        [smem] * 4 + [vmem] * 3 + [hbm] * 2,
        (vmem, vmem, hbm, hbm, vmem),
        scratch_shapes=[
            pltpu.VMEM((2, *flat), bf16),
            pltpu.VMEM(flat[1:], f32),
            pltpu.SemaphoreType.DMA((4,)),
        ],
        room=8,
    )(
        past_lengths,
        accepted,
        parents,
        lambda_head,
        query_gain[None],
        key_gain[None],
        head_gain[None],
        cache_keys.reshape(flat),
        cache_values.reshape(flat),
    )
    query, row = call(
        finish_rows,
        (shape((nears, chunk, width), bf16), shape((8, 128), bf16)),
        [vmem] * 2,
        (vmem, vmem),
    )(shared, facts)
    query = lax.all_to_all(query, near, 0, 0, tiled=True).reshape(tokens, width)
    part = call(
        attend, shape((nears, tps, 24, 128), bf16), [vmem] * 5, flops=10000000, room=16
    )(facts, query, row, keys, values)
    part = lax.all_to_all(
        part.reshape(nears * tps, 24, 128), (*near, tp), 0, 0, tiled=True
    )
    part = call(
        combine_near,
        shape((fars, 80, 128), bf16),
        [vmem, vmem],
        scratch_shapes=[pltpu.VMEM((128, 128), f32)],
    )(part.reshape(nears, tps, 24, 128), row)
    part = lax.all_to_all(part, far, 0, 0, tiled=True)
    mixed = call(combine_far, shape((nears, 96, 128), bf16), [vmem] * 2)(part, head_gain[None])
    mixed = lax.all_to_all(mixed, near, 0, 0, tiled=True)
    own = w_output.T
    weights = [own]
    for k in range(1, tps):
        ring = [(i, (i + k) % tps) for i in range(tps)]
        weights.append(lax.ppermute(own, tp, ring))
    whole = cache_keys.shape
    return call(
        finish,
        (
            shape((proposals, w_output.shape[1]), bf16),
            shape(whole, bf16),
            shape(whole, bf16),
        ),
        [hbm] * 2 + [vmem] * 5 + [hbm] * 2,
        (vmem, hbm, hbm),
        scratch_shapes=[
            pltpu.VMEM((256, 128), f32),
            pltpu.VMEM((proposals, heads, 128), bf16),
            pltpu.VMEM((proposals, heads, 128), bf16),
            pltpu.SMEM((2, seqs), jnp.int32),
            pltpu.SemaphoreType.DMA((2,)),
        ],
        input_output_aliases={7: 1, 8: 2},
    )(past_lengths, accepted, mixed, *weights, keys_copy.reshape(whole), values_copy.reshape(whole))


def solution(mesh):
    groups, shards, tps = (mesh.shape[a] for a in ("grp", "kv", "tp"))
    split = (groups, shards // (near_chips * near_cores), near_chips, near_cores, tps)
    finer = Mesh(mesh.devices.reshape(split), ("grp", far, chip, core, tp))
    kv = (far, chip, core)
    cache = P("grp", kv, tp, None)
    placed = (
        P("grp", kv),
        P(kv, tp),
        P(kv, tp),
        P(kv, tp),
        P(),
        P(),
        P(tp),
        P(),
        P(tp, kv),
        cache,
        cache,
        P("grp"),
        P("grp"),
        P("grp", None),
    )
    return jax.shard_map(
        on_device,
        mesh=finer,
        in_specs=placed,
        out_specs=(P(("grp", tp), kv), cache, cache),
        check_vma=False,
    )
```

```python
import functools
import math

import jax
import jax.numpy as jnp
from jax import lax
from jax.experimental import pallas as pl
from jax.experimental.pallas import tpu as pltpu
from jax.sharding import Mesh
from jax.sharding import PartitionSpec as P


epsilon = 1e-06
floor_value = -1e30
f32 = jnp.float32
bf16 = jnp.bfloat16
interpreted = False
near_chips = 4
near_cores = 2
half, quarter, chip, core, tp = "half", "quarter", "chip", "core", "tp"
far = (half, quarter)
listed = (quarter, half)
near = (chip, core)
near_terms = 2
far_terms = 2
rows = 128

vmem = pl.BlockSpec(memory_space=pltpu.VMEM)
smem = pl.BlockSpec(memory_space=pltpu.SMEM)
hbm = pl.BlockSpec(memory_space=pltpu.HBM)


def near_place():
    return lax.axis_index(chip) * lax.axis_size(core) + lax.axis_index(core)


def iota(shape, dim):
    return lax.broadcasted_iota(jnp.int32, shape, dim)


def call(body, out_shape, in_specs, out_specs=vmem, flops=1000000, room=4, **rest):
    return pl.pallas_call(
        body,
        out_shape=out_shape,
        in_specs=in_specs,
        out_specs=out_specs,
        interpret=interpreted,
        compiler_params=pltpu.CompilerParams(vmem_limit_bytes=int(room * 1024) << 10),
        cost_estimate=pl.CostEstimate(flops=flops, bytes_accessed=1000000, transcendentals=0),
        **rest,
    )


def terms_of(x, count):
    terms = []
    for _ in range(count):
        terms.append(x.astype(bf16))
        x = x - terms[-1].astype(f32)
    return terms


def parts_of(x):
    high = x.astype(bf16).astype(f32)
    middle = (x - high).astype(bf16).astype(f32)
    return high, middle, x - high - middle


def project(hidden_ref, query_ref, key_ref, value_ref, out_ref, hidden, weights, sems):
    width = query_ref.shape[1]
    copies = [pltpu.make_async_copy(hidden_ref, hidden, sems.at[3])]
    for k, ref in enumerate((query_ref, key_ref, value_ref)):
        copies.append(pltpu.make_async_copy(ref, weights.at[k], sems.at[k]))
    for c in copies:
        c.start()
    at = 0
    copies[0].wait()
    for k, count in enumerate((near_terms, 1, 1)):
        copies[k + 1].wait()
        sums = jnp.dot(hidden[...], weights[k], preferred_element_type=f32)
        for term in terms_of(sums, count):
            out_ref[:, at : at + width] = term
            at += width


def arrived_sum(arrived_ref, width, terms):
    total = arrived_ref[0].astype(f32)
    for k in range(1, arrived_ref.shape[0]):
        total = total + arrived_ref[k].astype(f32)
    query = total[:, :width]
    for k in range(1, terms):
        query = query + total[:, k * width : (k + 1) * width]
    return query, total[:, terms * width :]


def sum_near(arrived_ref, out_ref, *, width, order):
    query, rest = arrived_sum(arrived_ref, width, near_terms)
    terms = terms_of(query, far_terms)
    for k, to in enumerate(order):
        for i, term in enumerate(terms):
            out_ref[k, :, i * width : (i + 1) * width] = term
        row = [rest[to : to + 1, 128 * i : 128 * (i + 1)] for i in range(8)]
        out_ref[k, :, far_terms * width :] = jnp.concatenate(row, axis=0).astype(bf16)


def normed(x, gain, lane, half):
    squares = x * x
    first = jnp.sum(jnp.where(lane < half, squares, 0.0), axis=-1, keepdims=True)
    second = jnp.sum(jnp.where(lane < half, 0.0, squares), axis=-1, keepdims=True)
    mean = jnp.where(lane < half, first, second) / half
    return x * lax.rsqrt(mean + epsilon) * gain


def finish_rows(arrived_ref, facts_ref, query_ref, row_ref):
    gains = facts_ref[facts_ref.shape[0] - 8 :]
    width = query_ref.shape[2]
    total, row = arrived_sum(arrived_ref, width, far_terms)
    lane = iota((8, 128), 1)
    query_gain, key_gain = gains[0:1], gains[1:2]
    for i in range(width // 128):
        at = slice(128 * i, 128 * (i + 1))
        part = normed(total[:, at], query_gain, lane, 64).astype(bf16)
        for k in range(query_ref.shape[0]):
            query_ref[k, :, at] = part
    row = jnp.where(iota((8, 128), 0) < 4, normed(row, key_gain, lane, 64), row)
    row_ref[...] = row.astype(bf16)


def stage(
    past_ref,
    accepted_ref,
    parents_ref,
    lambda_ref,
    query_gain_ref,
    key_gain_ref,
    head_gain_ref,
    keys_ref,
    values_ref,
    keys_vmem_ref,
    values_vmem_ref,
    keys_out_ref,
    values_out_ref,
    facts_ref,
    raw,
    wide,
    sems,
):
    taken = [
        pltpu.make_async_copy(keys_ref, raw.at[0], sems.at[0]),
        pltpu.make_async_copy(values_ref, raw.at[1], sems.at[1]),
    ]
    put = [
        pltpu.make_async_copy(raw.at[0], keys_out_ref, sems.at[2]),
        pltpu.make_async_copy(raw.at[1], values_out_ref, sems.at[3]),
    ]
    for c in taken:
        c.start()
    seqs, proposals = parents_ref.shape
    nears = lax.axis_size(near)
    far_index = lax.axis_index(far)
    own = near_place() * (seqs * proposals // nears) + far_index
    offset = (far_index * nears + near_place()) * (keys_ref.shape[1] // 4)
    own_seq, own_order = own // proposals, lax.rem(own, proposals)
    below = jnp.int32(0)
    for j in range(proposals):
        parent = parents_ref[own_seq, j]
        above = jnp.where(parent >= 0, (below >> jnp.maximum(parent, 0)) & 1, 0)
        below = below | (jnp.where(own_order == j, 1, above) << j)
    row = iota((rows, 128), 0)
    under = (below >> (2 * ((row >> 2) & 7) + (row & 1))) & 1
    limit = jnp.zeros((8, 128), jnp.int32)
    for s in range(seqs):
        limit = jnp.where(iota((8, 128), 0) == s, past_ref[s] + accepted_ref[s] - offset, limit)
        facts_ref[rows * s : rows * (s + 1)] = jnp.where(own_seq == s, under, 0).astype(f32)
    scale = jnp.ones((rows, 128), f32)
    for h in range(4):
        scale = jnp.where(((row >> 5) == h) & (((row >> 1) & 1) == 1), lambda_ref[h], scale)
    facts_ref[rows * seqs : rows * (seqs + 1)] = scale
    last = rows * (seqs + 1)
    facts_ref[last : last + 8] = limit.astype(f32)
    gains = [jnp.concatenate([ref[...]] * 2, axis=1) for ref in (query_gain_ref, key_gain_ref)]
    gains += [head_gain_ref[...], jnp.zeros((5, 128), f32)]
    facts_ref[last + 8 :] = jnp.concatenate(gains, axis=0)
    heads = keys_vmem_ref.shape[0] // seqs
    for k, out_ref in enumerate((keys_vmem_ref, values_vmem_ref)):
        taken[k].wait()
        put[k].start()
        for q in range(seqs):
            wide[...] = raw[k, q].astype(f32)
            for h in range(heads):
                part = wide[pl.ds(h, out_ref.shape[1], stride=heads), :]
                out_ref[q * heads + h] = part.astype(bf16)
    for d in put:
        d.wait()


def attend(
    facts_ref,
    query_ref,
    row_ref,
    keys_ref,
    values_ref,
    out_ref,
):
    seqs = out_ref.shape[1]
    heads = keys_ref.shape[0] // seqs
    positions_dev = keys_ref.shape[1]
    proposals = query_ref.shape[0] // seqs
    count = rows // heads
    line = iota((count, 128), 0)
    line_order = 2 * (line >> 2) + (line & 1)
    spread = (iota((count, proposals), 1) == line_order[:, :proposals]).astype(bf16)
    comp_at = (iota((count, 128), 1) >= 64) == (((line >> 1) & 1) == 1)
    row = iota((rows, rows), 0)
    lane = iota((rows, rows), 1)
    sent = (lane == count * (row & 3) + (row >> 2)).astype(bf16)
    last = rows * (seqs + 1)
    limits = facts_ref[last : last + 8]
    scale = facts_ref[rows * seqs : last]
    position = iota((rows, positions_dev), 1).astype(f32)
    new_row = row_ref[...].astype(f32)
    new_key, new_value = (
        jnp.concatenate(
            [jnp.broadcast_to(new_row[h : h + 1], (count, 128)) for h in at], axis=0
        )
        for at in (range(heads), range(heads, 2 * heads))
    )
    every = range(seqs)
    parts = [slice(count * h, count * (h + 1)) for h in range(heads)]
    wide = [
        jnp.dot(
            spread, query_ref[s * proposals : (s + 1) * proposals, :], preferred_element_type=f32
        )
        for s in every
    ]
    query = [
        jnp.concatenate(
            [jnp.where(comp_at, wide[s][:, 128 * h : 128 * (h + 1)], 0.0) for h in range(heads)],
            axis=0,
        )
        for s in every
    ]
    scores = [
        jnp.concatenate(
            [
                lax.dot_general(
                    query[s][parts[h]].astype(bf16),
                    keys_ref[s * heads + h],
                    (((1,), (1,)), ((), ())),
                    preferred_element_type=f32,
                )
                for h in range(heads)
            ],
            axis=0,
        )
        for s in every
    ]
    tree = [jnp.sum(query[s] * new_key, axis=-1, keepdims=True) * 0.125 for s in every]
    visible = [
        position < jnp.minimum(limits[s : s + 1, :1], float(positions_dev)) for s in every
    ]
    tree_visible = [facts_ref[rows * s : rows * (s + 1), :1] > 0.5 for s in every]
    masked = [jnp.where(visible[s], scores[s] * 0.125, floor_value) for s in every]
    tree = [jnp.where(tree_visible[s], tree[s], floor_value) for s in every]
    top = [jnp.maximum(jnp.max(masked[s], axis=-1, keepdims=True), tree[s]) for s in every]
    weights = [jnp.where(visible[s], jnp.exp(masked[s] - top[s]), 0.0) for s in every]
    tree_weight = [jnp.where(tree_visible[s], jnp.exp(tree[s] - top[s]), 0.0) for s in every]
    total = [jnp.sum(weights[s], axis=-1, keepdims=True) + tree_weight[s] for s in every]
    acc = [
        jnp.concatenate(
            [
                jnp.dot(
                    weights[s][parts[h]].astype(bf16),
                    values_ref[s * heads + h],
                    preferred_element_type=f32,
                )
                for h in range(heads)
            ],
            axis=0,
        )
        for s in every
    ]
    acc = [
        (acc[s] + tree_weight[s].astype(bf16).astype(f32) * new_value) * scale for s in every
    ]
    stats = []
    for s in every:
        stat = jnp.zeros((rows, 128), f32)
        for k, part in enumerate((*parts_of(top[s]), *parts_of(total[s]))):
            stat = jnp.where(lane == k, part, stat)
        stats.append(stat)
    both = [
        jnp.dot(
            sent,
            jnp.concatenate([acc[s].astype(bf16), stats[s].astype(bf16)], axis=1),
            preferred_element_type=f32,
        )
        for s in every
    ]
    stats = [jnp.transpose(both[s][:, 128:])[:8].astype(bf16) for s in every]
    for s in every:
        sums = both[s][:, :128].astype(bf16)
        for r in range(out_ref.shape[0]):
            out_ref[r, s, :16, :] = sums[16 * r : 16 * (r + 1)]
            out_ref[r, s, 16:, :] = stats[s]


def stat_rows(stats):
    return stats[0:1] + stats[1:2] + stats[2:3], stats[3:4] + stats[4:5] + stats[5:6]


def combine_near(arrived_ref, row_ref, out_ref, factor_ref):
    me = near_place()
    sources, groups = arrived_ref.shape[:2]
    tiles, factors = [], []
    lane = iota((8, 128), 1)
    packed = jnp.zeros((8, 128), f32)
    for g in range(groups):
        tops, sums = zip(*[stat_rows(arrived_ref[r, g, 16:, :].astype(f32)) for r in range(sources)])
        top = functools.reduce(jnp.maximum, tops)
        scales = [jnp.exp(t - top) for t in tops]
        total = sum(s * f for s, f in zip(sums, scales))
        factors.extend(scales)
        zero = jnp.zeros((1, 128), f32)
        stats = jnp.concatenate([*parts_of(top), *parts_of(total), zero, zero], axis=0)
        moved = pltpu.roll(stats, lax.rem(128 + 16 * g - 16 * me, 128), 1)
        packed = jnp.where((lane >> 4) == g, moved, packed)
    count = sources * groups
    wide = jnp.concatenate(factors + [jnp.zeros((128 - count, 128), f32)], axis=0)
    factor_ref[...] = jnp.transpose(wide)
    mine = factor_ref[pl.ds(pl.multiple_of(16 * me, 16), 16), :]
    for g in range(groups):
        acc = jnp.zeros((16, 128), f32)
        for r in range(sources):
            at = g * sources + r
            acc = acc + arrived_ref[r, g, :16, :].astype(f32) * mine[:, at : at + 1]
        tiles.append(acc.astype(bf16))
    for k in range(out_ref.shape[0]):
        for g in range(groups):
            out_ref[k, 16 * g : 16 * (g + 1), :] = tiles[g]
        out_ref[k, 64:72, :] = packed.astype(bf16)
        out_ref[k, 72:80, :] = row_ref[...]


def combine_far(arrived_ref, gain_ref, out_ref, *, order):
    sources = arrived_ref.shape[0]
    tops, sums = zip(*[stat_rows(arrived_ref[q, 64:72, :].astype(f32)) for q in range(sources)])
    top = functools.reduce(jnp.maximum, tops)
    scales = [jnp.exp(t - top) for t in tops]
    total = sum(s * f for s, f in zip(sums, scales))
    wide = jnp.concatenate(scales + [total, jnp.zeros((127 - sources, 128), f32)], axis=0)
    columns = jnp.transpose(wide)[:64]
    acc = jnp.zeros((64, 128), f32)
    for q in range(sources):
        acc = acc + arrived_ref[q, :64, :].astype(f32) * columns[:, q : q + 1]
    acc = acc / columns[:, sources : sources + 1]
    heads = []
    for g in range(4):
        mixture = acc[16 * g : 16 * g + 8] - acc[16 * g + 8 : 16 * g + 16]
        mean = jnp.mean(mixture * mixture, axis=-1, keepdims=True)
        heads.append((mixture * lax.rsqrt(mean + epsilon) * gain_ref[...]).astype(bf16))
    for k in range(out_ref.shape[0]):
        for g in range(4):
            out_ref[k, 8 * g : 8 * (g + 1), :] = heads[g]
        for q, source in enumerate(order):
            at = 32 + 8 * source
            out_ref[k, at : at + 8, :] = arrived_ref[q, 72:80, :]


def finish(
    past_ref,
    accepted_ref,
    arrived_ref,
    own_ref,
    first_ref,
    second_ref,
    third_ref,
    keys_ref,
    values_ref,
    out_ref,
    keys_out_ref,
    values_out_ref,
    heads_ref,
    key_rows,
    value_rows,
    lengths,
    sem,
):
    known = [
        pltpu.make_async_copy(past_ref, lengths.at[0], sem.at[0]),
        pltpu.make_async_copy(accepted_ref, lengths.at[1], sem.at[1]),
    ]
    for c in known:
        c.start()
    del keys_ref, values_ref
    sources = arrived_ref.shape[0]
    heads = jnp.concatenate([arrived_ref[r, :32, :] for r in range(sources)], axis=0)
    count = heads.shape[0]
    to = iota((count, count), 0)
    source = ((to >> 1) & 7) * 32 + (to >> 6) * 8 + (to & 1) * 4 + ((to >> 4) & 3)
    order = (iota((count, count), 1) == source).astype(bf16)
    heads_ref[...] = jnp.dot(order, heads, preferred_element_type=f32)
    total = jnp.zeros(out_ref.shape, f32)
    for k, weight_ref in enumerate((own_ref, first_ref, second_ref, third_ref)):
        g = lax.rem(lax.axis_index(tp) + 4 - k, 4)
        mine = heads_ref[pl.ds(pl.multiple_of(64 * g, 64), 64), :].astype(bf16)
        left = jnp.concatenate([mine[16 * h : 16 * (h + 1)] for h in range(4)], axis=1)
        group = lax.dot_general(
            left, weight_ref[...], (((1,), (1,)), ((), ())), preferred_element_type=f32
        )
        total = total + group.astype(bf16).astype(f32)
    out_ref[...] = total.astype(bf16)
    for c in known:
        c.wait()
    seqs, positions_dev = keys_out_ref.shape[:2]
    offset = (lax.axis_index(far) * lax.axis_size(near) + near_place()) * positions_dev
    proposals = key_rows.shape[0]
    for s in range(seqs):
        first = lengths[0, s] + lengths[1, s] - offset

        @pl.when((first > -proposals) & (first < positions_dev))
        def _():
            for j in range(proposals):
                r, q = divmod(s * proposals + j, sources)
                key_rows[j] = arrived_ref[r, 32 + 8 * q : 36 + 8 * q, :]
                value_rows[j] = arrived_ref[r, 36 + 8 * q : 40 + 8 * q, :]
            for j in range(proposals):

                @pl.when((first + j >= 0) & (first + j < positions_dev))
                def _():
                    at = jnp.clip(first + j, 0, positions_dev - 1)
                    writes = [
                        pltpu.make_async_copy(rows.at[j], whole.at[s, at], sem.at[k])
                        for k, (rows, whole) in enumerate(
                            ((key_rows, keys_out_ref), (value_rows, values_out_ref))
                        )
                    ]
                    for c in writes:
                        c.start()
                    for c in writes:
                        c.wait()


def on_device(
    hidden_states,
    w_query,
    w_key,
    w_value,
    query_gain,
    key_gain,
    lambda_head,
    head_gain,
    w_output,
    cache_keys,
    cache_values,
    past_lengths,
    accepted,
    parents,
):
    shape = jax.ShapeDtypeStruct
    seqs, proposals = parents.shape
    tokens = hidden_states.shape[0]
    width = w_query.shape[1]
    positions_dev, heads = cache_keys.shape[1:3]
    nears, fars, tps = (math.prod(lax.axis_size(a) for a in axes) for axes in (near, far, (tp,)))
    chunk = tokens // nears
    halves = lax.axis_size(half)
    order = [(k % halves) * (fars // halves) + k // halves for k in range(fars)]
    terms = call(
        project,
        shape((tokens, (near_terms + 2) * width), bf16),
        [hbm] * 4,
        room=65182 / 1024,
        scratch_shapes=[
            pltpu.VMEM(hidden_states.shape, bf16),
            pltpu.VMEM((3, *w_query.shape), bf16),
            pltpu.SemaphoreType.DMA((4,)),
        ],
    )(hidden_states, w_query, w_key, w_value)
    terms = lax.all_to_all(
        terms.reshape(nears, chunk, -1), near, 0, 0, tiled=True
    )
    shared = call(
        functools.partial(sum_near, width=width, order=order),
        shape((fars, chunk, far_terms * width + 128), bf16),
        [vmem],
    )(terms)
    shared = lax.all_to_all(shared, listed, 0, 0, tiled=True)
    flat = (seqs, positions_dev * heads, 128)
    keys, values, keys_copy, values_copy, facts = call(
        stage,
        (
            *[shape((seqs * heads, positions_dev, 128), bf16)] * 2,
            *[shape(flat, bf16)] * 2,
            shape((rows * (seqs + 1) + 16, 128), f32),
        ),
        [smem] * 4 + [vmem] * 3 + [hbm] * 2,
        (vmem, vmem, hbm, hbm, vmem),
        scratch_shapes=[
            pltpu.VMEM((2, *flat), bf16),
            pltpu.VMEM(flat[1:], f32),
            pltpu.SemaphoreType.DMA((4,)),
        ],
        room=8,
    )(
        past_lengths,
        accepted,
        parents,
        lambda_head,
        query_gain[None],
        key_gain[None],
        head_gain[None],
        cache_keys.reshape(flat),
        cache_values.reshape(flat),
    )
    query, row = call(
        finish_rows,
        (shape((nears, chunk, width), bf16), shape((8, 128), bf16)),
        [vmem] * 2,
        (vmem, vmem),
    )(shared, facts)
    query = lax.all_to_all(query, near, 0, 0, tiled=True).reshape(tokens, width)
    part = call(
        attend, shape((nears, tps, 24, 128), bf16), [vmem] * 5, flops=10000000, room=16
    )(facts, query, row, keys, values)
    part = lax.all_to_all(
        part.reshape(nears * tps, 24, 128), (*near, tp), 0, 0, tiled=True
    )
    part = call(
        combine_near,
        shape((fars, 80, 128), bf16),
        [vmem, vmem],
        scratch_shapes=[pltpu.VMEM((128, 128), f32)],
    )(part.reshape(nears, tps, 24, 128), row)
    part = lax.all_to_all(part, listed, 0, 0, tiled=True)
    mixed = call(
        functools.partial(combine_far, order=order), shape((nears, 96, 128), bf16), [vmem] * 2
    )(part, head_gain[None])
    mixed = lax.all_to_all(mixed, near, 0, 0, tiled=True)
    own = w_output.T
    weights = [own]
    for k in range(1, tps):
        ring = [(i, (i + k) % tps) for i in range(tps)]
        weights.append(lax.ppermute(own, tp, ring))
    whole = cache_keys.shape
    return call(
        finish,
        (
            shape((proposals, w_output.shape[1]), bf16),
            shape(whole, bf16),
            shape(whole, bf16),
        ),
        [hbm] * 2 + [vmem] * 5 + [hbm] * 2,
        (vmem, hbm, hbm),
        scratch_shapes=[
            pltpu.VMEM((256, 128), f32),
            pltpu.VMEM((proposals, heads, 128), bf16),
            pltpu.VMEM((proposals, heads, 128), bf16),
            pltpu.SMEM((2, seqs), jnp.int32),
            pltpu.SemaphoreType.DMA((2,)),
        ],
        input_output_aliases={7: 1, 8: 2},
    )(past_lengths, accepted, mixed, *weights, keys_copy.reshape(whole), values_copy.reshape(whole))


def solution(mesh):
    groups, shards, tps = (mesh.shape[a] for a in ("grp", "kv", "tp"))
    split = (groups, 2, shards // (2 * near_chips * near_cores), near_chips, near_cores, tps)
    finer = Mesh(mesh.devices.reshape(split), ("grp", half, quarter, chip, core, tp))
    kv = (half, quarter, chip, core)
    cache = P("grp", kv, tp, None)
    placed = (
        P("grp", kv),
        P(kv, tp),
        P(kv, tp),
        P(kv, tp),
        P(),
        P(),
        P(tp),
        P(),
        P(tp, kv),
        cache,
        cache,
        P("grp"),
        P("grp"),
        P("grp", None),
    )
    return jax.shard_map(
        on_device,
        mesh=finer,
        in_specs=placed,
        out_specs=(P(("grp", tp), kv), cache, cache),
        check_vma=False,
    )
```

```python
import functools
import math

import jax
import jax.numpy as jnp
from jax import lax
from jax.experimental import pallas as pl
from jax.experimental.pallas import tpu as pltpu
from jax.sharding import Mesh
from jax.sharding import PartitionSpec as P


epsilon = 1e-06
floor_value = -1e30
f32 = jnp.float32
bf16 = jnp.bfloat16
interpreted = False
near_chips = 4
near_cores = 2
half, quarter, eighth, chip, core, tp = "half", "quarter", "eighth", "chip", "core", "tp"
far = (half, quarter, eighth)
first_list = (eighth, quarter, half)
second_list = (eighth, quarter, half)
near = (chip, core)
near_terms = 2
far_terms = 2
rows = 128

vmem = pl.BlockSpec(memory_space=pltpu.VMEM)
smem = pl.BlockSpec(memory_space=pltpu.SMEM)
hbm = pl.BlockSpec(memory_space=pltpu.HBM)


def near_place():
    return lax.axis_index(chip) * lax.axis_size(core) + lax.axis_index(core)


def blocks_of(axes):
    blocks = []
    for k in range(math.prod(lax.axis_size(a) for a in axes)):
        at = {}
        for a in reversed(axes):
            k, at[a] = divmod(k, lax.axis_size(a))
        block = 0
        for a in far:
            block = block * lax.axis_size(a) + at[a]
        blocks.append(block)
    return blocks


def iota(shape, dim):
    return lax.broadcasted_iota(jnp.int32, shape, dim)


def call(body, out_shape, in_specs, out_specs=vmem, flops=1000000, room=4, **rest):
    return pl.pallas_call(
        body,
        out_shape=out_shape,
        in_specs=in_specs,
        out_specs=out_specs,
        interpret=interpreted,
        compiler_params=pltpu.CompilerParams(vmem_limit_bytes=int(room * 1024) << 10),
        cost_estimate=pl.CostEstimate(flops=flops, bytes_accessed=1000000, transcendentals=0),
        **rest,
    )


def terms_of(x, count):
    terms = []
    for _ in range(count):
        terms.append(x.astype(bf16))
        x = x - terms[-1].astype(f32)
    return terms


def parts_of(x):
    high = x.astype(bf16).astype(f32)
    middle = (x - high).astype(bf16).astype(f32)
    return high, middle, x - high - middle


def project(hidden_ref, query_ref, key_ref, value_ref, out_ref, hidden, weights, sems):
    width = query_ref.shape[1]
    copies = [pltpu.make_async_copy(hidden_ref, hidden, sems.at[3])]
    for k, ref in enumerate((query_ref, key_ref, value_ref)):
        copies.append(pltpu.make_async_copy(ref, weights.at[k], sems.at[k]))
    for c in copies:
        c.start()
    at = 0
    copies[0].wait()
    for k, count in enumerate((near_terms, 1, 1)):
        copies[k + 1].wait()
        sums = jnp.dot(hidden[...], weights[k], preferred_element_type=f32)
        for term in terms_of(sums, count):
            out_ref[:, at : at + width] = term
            at += width


def arrived_sum(arrived_ref, width, terms):
    total = arrived_ref[0].astype(f32)
    for k in range(1, arrived_ref.shape[0]):
        total = total + arrived_ref[k].astype(f32)
    query = total[:, :width]
    for k in range(1, terms):
        query = query + total[:, k * width : (k + 1) * width]
    return query, total[:, terms * width :]


def sum_near(arrived_ref, out_ref, *, width, order):
    query, rest = arrived_sum(arrived_ref, width, near_terms)
    terms = terms_of(query, far_terms)
    for k, to in enumerate(order):
        for i, term in enumerate(terms):
            out_ref[k, :, i * width : (i + 1) * width] = term
        row = [rest[to : to + 1, 128 * i : 128 * (i + 1)] for i in range(8)]
        out_ref[k, :, far_terms * width :] = jnp.concatenate(row, axis=0).astype(bf16)


def normed(x, gain, lane, half):
    squares = x * x
    first = jnp.sum(jnp.where(lane < half, squares, 0.0), axis=-1, keepdims=True)
    second = jnp.sum(jnp.where(lane < half, 0.0, squares), axis=-1, keepdims=True)
    mean = jnp.where(lane < half, first, second) / half
    return x * lax.rsqrt(mean + epsilon) * gain


def finish_rows(arrived_ref, facts_ref, query_ref, row_ref):
    gains = facts_ref[facts_ref.shape[0] - 8 :]
    width = query_ref.shape[2]
    total, row = arrived_sum(arrived_ref, width, far_terms)
    lane = iota((8, 128), 1)
    query_gain, key_gain = gains[0:1], gains[1:2]
    for i in range(width // 128):
        at = slice(128 * i, 128 * (i + 1))
        part = normed(total[:, at], query_gain, lane, 64).astype(bf16)
        for k in range(query_ref.shape[0]):
            query_ref[k, :, at] = part
    row = jnp.where(iota((8, 128), 0) < 4, normed(row, key_gain, lane, 64), row)
    row_ref[...] = row.astype(bf16)


def stage(
    past_ref,
    accepted_ref,
    parents_ref,
    lambda_ref,
    query_gain_ref,
    key_gain_ref,
    head_gain_ref,
    keys_ref,
    values_ref,
    keys_vmem_ref,
    values_vmem_ref,
    keys_out_ref,
    values_out_ref,
    facts_ref,
    raw,
    wide,
    sems,
):
    taken = [
        pltpu.make_async_copy(keys_ref, raw.at[0], sems.at[0]),
        pltpu.make_async_copy(values_ref, raw.at[1], sems.at[1]),
    ]
    put = [
        pltpu.make_async_copy(raw.at[0], keys_out_ref, sems.at[2]),
        pltpu.make_async_copy(raw.at[1], values_out_ref, sems.at[3]),
    ]
    for c in taken:
        c.start()
    seqs, proposals = parents_ref.shape
    nears = lax.axis_size(near)
    far_index = lax.axis_index(far)
    own = near_place() * (seqs * proposals // nears) + far_index
    offset = (far_index * nears + near_place()) * (keys_ref.shape[1] // 4)
    own_seq, own_order = own // proposals, lax.rem(own, proposals)
    below = jnp.int32(0)
    for j in range(proposals):
        parent = parents_ref[own_seq, j]
        above = jnp.where(parent >= 0, (below >> jnp.maximum(parent, 0)) & 1, 0)
        below = below | (jnp.where(own_order == j, 1, above) << j)
    row = iota((rows, 128), 0)
    under = (below >> (2 * ((row >> 2) & 7) + (row & 1))) & 1
    limit = jnp.zeros((8, 128), jnp.int32)
    for s in range(seqs):
        limit = jnp.where(iota((8, 128), 0) == s, past_ref[s] + accepted_ref[s] - offset, limit)
        facts_ref[rows * s : rows * (s + 1)] = jnp.where(own_seq == s, under, 0).astype(f32)
    scale = jnp.ones((rows, 128), f32)
    for h in range(4):
        scale = jnp.where(((row >> 5) == h) & (((row >> 1) & 1) == 1), lambda_ref[h], scale)
    facts_ref[rows * seqs : rows * (seqs + 1)] = scale
    last = rows * (seqs + 1)
    facts_ref[last : last + 8] = limit.astype(f32)
    gains = [jnp.concatenate([ref[...]] * 2, axis=1) for ref in (query_gain_ref, key_gain_ref)]
    gains += [head_gain_ref[...], jnp.zeros((5, 128), f32)]
    facts_ref[last + 8 :] = jnp.concatenate(gains, axis=0)
    heads = keys_vmem_ref.shape[0] // seqs
    for k, out_ref in enumerate((keys_vmem_ref, values_vmem_ref)):
        taken[k].wait()
        put[k].start()
        for q in range(seqs):
            wide[...] = raw[k, q].astype(f32)
            for h in range(heads):
                part = wide[pl.ds(h, out_ref.shape[1], stride=heads), :]
                out_ref[q * heads + h] = part.astype(bf16)
    for d in put:
        d.wait()


def attend(
    facts_ref,
    query_ref,
    row_ref,
    keys_ref,
    values_ref,
    out_ref,
):
    seqs = out_ref.shape[1]
    heads = keys_ref.shape[0] // seqs
    positions_dev = keys_ref.shape[1]
    proposals = query_ref.shape[0] // seqs
    count = rows // heads
    line = iota((count, 128), 0)
    line_order = 2 * (line >> 2) + (line & 1)
    spread = (iota((count, proposals), 1) == line_order[:, :proposals]).astype(bf16)
    comp_at = (iota((count, 128), 1) >= 64) == (((line >> 1) & 1) == 1)
    row = iota((rows, rows), 0)
    lane = iota((rows, rows), 1)
    sent = (lane == count * (row & 3) + (row >> 2)).astype(bf16)
    last = rows * (seqs + 1)
    limits = facts_ref[last : last + 8]
    scale = facts_ref[rows * seqs : last]
    position = iota((rows, positions_dev), 1).astype(f32)
    new_row = row_ref[...].astype(f32)
    new_key, new_value = (
        jnp.concatenate(
            [jnp.broadcast_to(new_row[h : h + 1], (count, 128)) for h in at], axis=0
        )
        for at in (range(heads), range(heads, 2 * heads))
    )
    every = range(seqs)
    parts = [slice(count * h, count * (h + 1)) for h in range(heads)]
    wide = [
        jnp.dot(
            spread, query_ref[s * proposals : (s + 1) * proposals, :], preferred_element_type=f32
        )
        for s in every
    ]
    query = [
        jnp.concatenate(
            [jnp.where(comp_at, wide[s][:, 128 * h : 128 * (h + 1)], 0.0) for h in range(heads)],
            axis=0,
        )
        for s in every
    ]
    scores = [
        jnp.concatenate(
            [
                lax.dot_general(
                    query[s][parts[h]].astype(bf16),
                    keys_ref[s * heads + h],
                    (((1,), (1,)), ((), ())),
                    preferred_element_type=f32,
                )
                for h in range(heads)
            ],
            axis=0,
        )
        for s in every
    ]
    tree = [jnp.sum(query[s] * new_key, axis=-1, keepdims=True) * 0.125 for s in every]
    visible = [
        position < jnp.minimum(limits[s : s + 1, :1], float(positions_dev)) for s in every
    ]
    tree_visible = [facts_ref[rows * s : rows * (s + 1), :1] > 0.5 for s in every]
    masked = [jnp.where(visible[s], scores[s] * 0.125, floor_value) for s in every]
    tree = [jnp.where(tree_visible[s], tree[s], floor_value) for s in every]
    top = [jnp.maximum(jnp.max(masked[s], axis=-1, keepdims=True), tree[s]) for s in every]
    weights = [jnp.where(visible[s], jnp.exp(masked[s] - top[s]), 0.0) for s in every]
    tree_weight = [jnp.where(tree_visible[s], jnp.exp(tree[s] - top[s]), 0.0) for s in every]
    total = [jnp.sum(weights[s], axis=-1, keepdims=True) + tree_weight[s] for s in every]
    acc = [
        jnp.concatenate(
            [
                jnp.dot(
                    weights[s][parts[h]].astype(bf16),
                    values_ref[s * heads + h],
                    preferred_element_type=f32,
                )
                for h in range(heads)
            ],
            axis=0,
        )
        for s in every
    ]
    acc = [
        (acc[s] + tree_weight[s].astype(bf16).astype(f32) * new_value) * scale for s in every
    ]
    stats = []
    for s in every:
        stat = jnp.zeros((rows, 128), f32)
        for k, part in enumerate((*parts_of(top[s]), *parts_of(total[s]))):
            stat = jnp.where(lane == k, part, stat)
        stats.append(stat)
    both = [
        jnp.dot(
            sent,
            jnp.concatenate([acc[s].astype(bf16), stats[s].astype(bf16)], axis=1),
            preferred_element_type=f32,
        )
        for s in every
    ]
    stats = [jnp.transpose(both[s][:, 128:])[:8].astype(bf16) for s in every]
    for s in every:
        sums = both[s][:, :128].astype(bf16)
        for r in range(out_ref.shape[0]):
            out_ref[r, s, :16, :] = sums[16 * r : 16 * (r + 1)]
            out_ref[r, s, 16:, :] = stats[s]


def stat_rows(stats):
    return stats[0:1] + stats[1:2] + stats[2:3], stats[3:4] + stats[4:5] + stats[5:6]


def combine_near(arrived_ref, row_ref, out_ref, factor_ref):
    me = near_place()
    sources, groups = arrived_ref.shape[:2]
    tiles, factors = [], []
    lane = iota((8, 128), 1)
    packed = jnp.zeros((8, 128), f32)
    for g in range(groups):
        tops, sums = zip(*[stat_rows(arrived_ref[r, g, 16:, :].astype(f32)) for r in range(sources)])
        top = functools.reduce(jnp.maximum, tops)
        scales = [jnp.exp(t - top) for t in tops]
        total = sum(s * f for s, f in zip(sums, scales))
        factors.extend(scales)
        zero = jnp.zeros((1, 128), f32)
        stats = jnp.concatenate([*parts_of(top), *parts_of(total), zero, zero], axis=0)
        moved = pltpu.roll(stats, lax.rem(128 + 16 * g - 16 * me, 128), 1)
        packed = jnp.where((lane >> 4) == g, moved, packed)
    count = sources * groups
    wide = jnp.concatenate(factors + [jnp.zeros((128 - count, 128), f32)], axis=0)
    factor_ref[...] = jnp.transpose(wide)
    mine = factor_ref[pl.ds(pl.multiple_of(16 * me, 16), 16), :]
    for g in range(groups):
        acc = jnp.zeros((16, 128), f32)
        for r in range(sources):
            at = g * sources + r
            acc = acc + arrived_ref[r, g, :16, :].astype(f32) * mine[:, at : at + 1]
        tiles.append(acc.astype(bf16))
    for k in range(out_ref.shape[0]):
        for g in range(groups):
            out_ref[k, 16 * g : 16 * (g + 1), :] = tiles[g]
        out_ref[k, 64:72, :] = packed.astype(bf16)
        out_ref[k, 72:80, :] = row_ref[...]


def combine_far(arrived_ref, gain_ref, out_ref, *, order):
    sources = arrived_ref.shape[0]
    tops, sums = zip(*[stat_rows(arrived_ref[q, 64:72, :].astype(f32)) for q in range(sources)])
    top = functools.reduce(jnp.maximum, tops)
    scales = [jnp.exp(t - top) for t in tops]
    total = sum(s * f for s, f in zip(sums, scales))
    wide = jnp.concatenate(scales + [total, jnp.zeros((127 - sources, 128), f32)], axis=0)
    columns = jnp.transpose(wide)[:64]
    acc = jnp.zeros((64, 128), f32)
    for q in range(sources):
        acc = acc + arrived_ref[q, :64, :].astype(f32) * columns[:, q : q + 1]
    acc = acc / columns[:, sources : sources + 1]
    heads = []
    for g in range(4):
        mixture = acc[16 * g : 16 * g + 8] - acc[16 * g + 8 : 16 * g + 16]
        mean = jnp.mean(mixture * mixture, axis=-1, keepdims=True)
        heads.append((mixture * lax.rsqrt(mean + epsilon) * gain_ref[...]).astype(bf16))
    for k in range(out_ref.shape[0]):
        for g in range(4):
            out_ref[k, 8 * g : 8 * (g + 1), :] = heads[g]
        for q, source in enumerate(order):
            at = 32 + 8 * source
            out_ref[k, at : at + 8, :] = arrived_ref[q, 72:80, :]


def finish(
    past_ref,
    accepted_ref,
    arrived_ref,
    own_ref,
    first_ref,
    second_ref,
    third_ref,
    keys_ref,
    values_ref,
    out_ref,
    keys_out_ref,
    values_out_ref,
    heads_ref,
    key_rows,
    value_rows,
    lengths,
    sem,
):
    known = [
        pltpu.make_async_copy(past_ref, lengths.at[0], sem.at[0]),
        pltpu.make_async_copy(accepted_ref, lengths.at[1], sem.at[1]),
    ]
    for c in known:
        c.start()
    del keys_ref, values_ref
    sources = arrived_ref.shape[0]
    heads = jnp.concatenate([arrived_ref[r, :32, :] for r in range(sources)], axis=0)
    count = heads.shape[0]
    to = iota((count, count), 0)
    source = ((to >> 1) & 7) * 32 + (to >> 6) * 8 + (to & 1) * 4 + ((to >> 4) & 3)
    order = (iota((count, count), 1) == source).astype(bf16)
    heads_ref[...] = jnp.dot(order, heads, preferred_element_type=f32)
    total = jnp.zeros(out_ref.shape, f32)
    for k, weight_ref in enumerate((own_ref, first_ref, second_ref, third_ref)):
        g = lax.rem(lax.axis_index(tp) + 4 - k, 4)
        mine = heads_ref[pl.ds(pl.multiple_of(64 * g, 64), 64), :].astype(bf16)
        left = jnp.concatenate([mine[16 * h : 16 * (h + 1)] for h in range(4)], axis=1)
        group = lax.dot_general(
            left, weight_ref[...], (((1,), (1,)), ((), ())), preferred_element_type=f32
        )
        total = total + group.astype(bf16).astype(f32)
    out_ref[...] = total.astype(bf16)
    for c in known:
        c.wait()
    seqs, positions_dev = keys_out_ref.shape[:2]
    offset = (lax.axis_index(far) * lax.axis_size(near) + near_place()) * positions_dev
    proposals = key_rows.shape[0]
    for s in range(seqs):
        first = lengths[0, s] + lengths[1, s] - offset

        @pl.when((first > -proposals) & (first < positions_dev))
        def _():
            for j in range(proposals):
                r, q = divmod(s * proposals + j, sources)
                key_rows[j] = arrived_ref[r, 32 + 8 * q : 36 + 8 * q, :]
                value_rows[j] = arrived_ref[r, 36 + 8 * q : 40 + 8 * q, :]
            for j in range(proposals):

                @pl.when((first + j >= 0) & (first + j < positions_dev))
                def _():
                    at = jnp.clip(first + j, 0, positions_dev - 1)
                    writes = [
                        pltpu.make_async_copy(rows.at[j], whole.at[s, at], sem.at[k])
                        for k, (rows, whole) in enumerate(
                            ((key_rows, keys_out_ref), (value_rows, values_out_ref))
                        )
                    ]
                    for c in writes:
                        c.start()
                    for c in writes:
                        c.wait()


def on_device(
    hidden_states,
    w_query,
    w_key,
    w_value,
    query_gain,
    key_gain,
    lambda_head,
    head_gain,
    w_output,
    cache_keys,
    cache_values,
    past_lengths,
    accepted,
    parents,
):
    shape = jax.ShapeDtypeStruct
    seqs, proposals = parents.shape
    tokens = hidden_states.shape[0]
    width = w_query.shape[1]
    positions_dev, heads = cache_keys.shape[1:3]
    nears, fars, tps = (math.prod(lax.axis_size(a) for a in axes) for axes in (near, far, (tp,)))
    chunk = tokens // nears
    first_order, second_order = (blocks_of(axes) for axes in (first_list, second_list))
    terms = call(
        project,
        shape((tokens, (near_terms + 2) * width), bf16),
        [hbm] * 4,
        room=65182 / 1024,
        scratch_shapes=[
            pltpu.VMEM(hidden_states.shape, bf16),
            pltpu.VMEM((3, *w_query.shape), bf16),
            pltpu.SemaphoreType.DMA((4,)),
        ],
    )(hidden_states, w_query, w_key, w_value)
    terms = lax.all_to_all(
        terms.reshape(nears, chunk, -1), near, 0, 0, tiled=True
    )
    shared = call(
        functools.partial(sum_near, width=width, order=first_order),
        shape((fars, chunk, far_terms * width + 128), bf16),
        [vmem],
    )(terms)
    shared = lax.all_to_all(shared, first_list, 0, 0, tiled=True)
    flat = (seqs, positions_dev * heads, 128)
    keys, values, keys_copy, values_copy, facts = call(
        stage,
        (
            *[shape((seqs * heads, positions_dev, 128), bf16)] * 2,
            *[shape(flat, bf16)] * 2,
            shape((rows * (seqs + 1) + 16, 128), f32),
        ),
        [smem] * 4 + [vmem] * 3 + [hbm] * 2,
        (vmem, vmem, hbm, hbm, vmem),
        scratch_shapes=[
            pltpu.VMEM((2, *flat), bf16),
            pltpu.VMEM(flat[1:], f32),
            pltpu.SemaphoreType.DMA((4,)),
        ],
        room=8,
    )(
        past_lengths,
        accepted,
        parents,
        lambda_head,
        query_gain[None],
        key_gain[None],
        head_gain[None],
        cache_keys.reshape(flat),
        cache_values.reshape(flat),
    )
    query, row = call(
        finish_rows,
        (shape((nears, chunk, width), bf16), shape((8, 128), bf16)),
        [vmem] * 2,
        (vmem, vmem),
    )(shared, facts)
    query = lax.all_to_all(query, near, 0, 0, tiled=True).reshape(tokens, width)
    part = call(
        attend, shape((nears, tps, 24, 128), bf16), [vmem] * 5, flops=10000000, room=16
    )(facts, query, row, keys, values)
    part = lax.all_to_all(
        part.reshape(nears * tps, 24, 128), (*near, tp), 0, 0, tiled=True
    )
    part = call(
        combine_near,
        shape((fars, 80, 128), bf16),
        [vmem, vmem],
        scratch_shapes=[pltpu.VMEM((128, 128), f32)],
    )(part.reshape(nears, tps, 24, 128), row)
    part = lax.all_to_all(part, second_list, 0, 0, tiled=True)
    mixed = call(
        functools.partial(combine_far, order=second_order),
        shape((nears, 96, 128), bf16),
        [vmem] * 2,
    )(part, head_gain[None])
    mixed = lax.all_to_all(mixed, near, 0, 0, tiled=True)
    own = w_output.T
    weights = [own]
    for k in range(1, tps):
        ring = [(i, (i + k) % tps) for i in range(tps)]
        weights.append(lax.ppermute(own, tp, ring))
    whole = cache_keys.shape
    return call(
        finish,
        (
            shape((proposals, w_output.shape[1]), bf16),
            shape(whole, bf16),
            shape(whole, bf16),
        ),
        [hbm] * 2 + [vmem] * 5 + [hbm] * 2,
        (vmem, hbm, hbm),
        scratch_shapes=[
            pltpu.VMEM((256, 128), f32),
            pltpu.VMEM((proposals, heads, 128), bf16),
            pltpu.VMEM((proposals, heads, 128), bf16),
            pltpu.SMEM((2, seqs), jnp.int32),
            pltpu.SemaphoreType.DMA((2,)),
        ],
        input_output_aliases={7: 1, 8: 2},
    )(past_lengths, accepted, mixed, *weights, keys_copy.reshape(whole), values_copy.reshape(whole))


def solution(mesh):
    groups, shards, tps = (mesh.shape[a] for a in ("grp", "kv", "tp"))
    split = (groups, 2, 2, shards // (4 * near_chips * near_cores), near_chips, near_cores, tps)
    finer = Mesh(mesh.devices.reshape(split), ("grp", half, quarter, eighth, chip, core, tp))
    kv = (half, quarter, eighth, chip, core)
    cache = P("grp", kv, tp, None)
    placed = (
        P("grp", kv),
        P(kv, tp),
        P(kv, tp),
        P(kv, tp),
        P(),
        P(),
        P(tp),
        P(),
        P(tp, kv),
        cache,
        cache,
        P("grp"),
        P("grp"),
        P("grp", None),
    )
    return jax.shard_map(
        on_device,
        mesh=finer,
        in_specs=placed,
        out_specs=(P(("grp", tp), kv), cache, cache),
        check_vma=False,
    )
```
